128 devices in a mesh: ep: 32 (over z, y, core), tp: 4 (over x).
Axes of the slice: x: 4, y: 4, z: 4, core: 2. Of those that a mesh axis runs over, the one named last changes fastest.
Arguments:
- tokens: bfloat16 [1536, 2048], P('ep'), may hold values from -6 to 6
- mix_gain: float32 [2048], replicated, may hold values from 0.1 to 1.9
- w_query: bfloat16 [2048, 1024], P(None, 'tp'), may hold values from -0.125 to 0.125
- w_key: bfloat16 [2048, 1024], P(None, 'tp'), may hold values from -0.125 to 0.125
- w_value: bfloat16 [2048, 1024], P(None, 'tp'), may hold values from -0.125 to 0.125
- w_outgate: bfloat16 [2048, 1024], P(None, 'tp'), may hold values from -0.125 to 0.125
- w_ingate: bfloat16 [2048, 8], P(None, 'tp'), may hold values from -0.125 to 0.125
- w_forget: bfloat16 [2048, 8], P(None, 'tp'), may hold values from -0.125 to 0.125
- in_bias: float32 [8], P('tp'), may hold values from -2 to 1
- forget_bias: float32 [8], P('tp'), may hold values from -1 to 4
- w_mix_out: bfloat16 [1024, 2048], replicated, may hold values from -0.1875 to 0.1875
- cell_state: float32 [1536, 8, 128, 128], P('ep', 'tp'), may hold values from -0.5 to 0.5
- norm_state: float32 [1536, 8, 128], P('ep', 'tp'), may hold values from -0.5 to 0.5
- max_state: float32 [1536, 8], P('ep', 'tp'), may hold values from -1 to 2
- moe_gain: float32 [2048], replicated, may hold values from 0.1 to 1.9
- route_ids: int32 [1536, 2], P('ep'), may hold values from 0 to 31, as said below
- route_weights: float32 [1536, 2], P('ep'), may hold values from 0.2 to 1
- expert_gate: bfloat16 [32, 2048, 1024], P('ep', None, 'tp'), may hold values from -0.125 to 0.125
- expert_up: bfloat16 [32, 2048, 1024], P('ep', None, 'tp'), may hold values from -0.125 to 0.125
- expert_down: bfloat16 [32, 1024, 2048], P('ep', 'tp'), may hold values from -0.1875 to 0.1875
- branch_gate: bfloat16 [2048], replicated, may hold values from -0.125 to 0.125
- dense_gate: bfloat16 [2048, 8192], P(None, ('ep', 'tp')), may hold values from -0.125 to 0.125
- dense_up: bfloat16 [2048, 8192], P(None, ('ep', 'tp')), may hold values from -0.125 to 0.125
- dense_down: bfloat16 [8192, 2048], P(('ep', 'tp')), may hold values from -0.25 to 0.25
Outputs:
- layer_out: bfloat16 [1536, 2048], P('ep', 'tp')
- new_cell: float32 [1536, 8, 128, 128], P('ep', 'tp')
- new_norm: float32 [1536, 8, 128], P('ep', 'tp')
- new_max: float32 [1536, 8], P('ep', 'tp')
The draws below stay inside these ranges and needn't reach their ends.
Inputs may be any that keep to these rules, and one draw needn't show every extreme that they name: `route_ids`: each row names two different experts of one group of 8 consecutive ids. Within the rows of one device no id appears more than 6 times, and some id appears exactly 6 times.
All inputs are finite; a program needn't handle non-finite values.
Results may differ from the reference program's by a relative error of at most 0.009.
The reference program's roundings to bfloat16 on the way count: a program that leaves them out, or rounds other values in their place, can miss the bound.
Values may be sent and summed in bfloat16 or wider, within the bound.
A program may use at most 128 MiB of HBM per device.

```python
import jax
import jax.numpy as jnp
from jax import lax

D = 2048
HEADS = 8
HD = 128
EXP_FF = 1024
DFF = 8192
GROUPS = 4
TOPK = 2
SEQ_DEV = 48
EXPERTS = 32
EXPERTS_PER_GROUP = 8
SEQS = 1536
CAP = 6
N_EP = 32


def draw_route_ids(key, part):
    block_count = SEQS // SEQ_DEV
    rand_keys = jax.random.split(key, 4)
    full_group = jax.random.randint(rand_keys[0], (block_count, 1), 0, GROUPS)
    other_group = (full_group + 1 + jax.random.randint(rand_keys[1], (block_count, SEQ_DEV), 0, GROUPS - 1)) % GROUPS
    position = jnp.arange(SEQ_DEV, dtype=jnp.int32)[None, :]
    group_ids = jnp.where(position < CAP * EXPERTS_PER_GROUP // 2, full_group, other_group)
    shuffle = jax.vmap(lambda row_key: jax.random.permutation(row_key, SEQ_DEV))(jax.random.split(rand_keys[2], block_count))
    group_ids = jnp.take_along_axis(group_ids, shuffle, axis=1)
    one_hot = (group_ids[:, :, None] == jnp.arange(GROUPS, dtype=jnp.int32)[None, None, :]).astype(jnp.int32)
    slot_rank = jnp.sum((jnp.cumsum(one_hot, axis=1) - 1) * one_hot, axis=2)
    offsets = jax.random.randint(rand_keys[3], (block_count, GROUPS), 0, EXPERTS_PER_GROUP)
    start_expert = jnp.take_along_axis(offsets, group_ids, axis=1)
    first_pick = (start_expert + 2 * slot_rank) % EXPERTS_PER_GROUP
    second_pick = (first_pick + 1) % EXPERTS_PER_GROUP
    group_base = group_ids * EXPERTS_PER_GROUP
    picks = jnp.stack([group_base + first_pick, group_base + second_pick], axis=-1)
    return picks.reshape(SEQS, 2).astype(jnp.int32)


def raised(entries, rng, source, target, parts, factor):
    def block_of(dim):
        return (jnp.arange(entries.shape[dim]) // (entries.shape[dim] // parts)).reshape((-1,) + (1,) * (entries.ndim - 1 - dim))

    first = jax.random.permutation(rng, parts)[block_of(target)]
    second = (block_of(target) + parts // 2) % parts
    return jnp.where((block_of(source) == first) | (block_of(source) == second), factor * entries, entries)


def block_levels(key, extent, cuts, least, high):
    loudness = 1.0
    for dim, blocks in cuts:
        steps = jax.random.uniform(jax.random.fold_in(jax.random.fold_in(key, 6), dim), (blocks,), jnp.float32, least / len(cuts), high / len(cuts))
        loudness = loudness * jnp.repeat(jnp.exp(steps), extent[dim] // blocks).reshape((-1,) + (1,) * (len(extent) - 1 - dim))
    return loudness


def gaussian(key, dims, width, bound, shards=(), kind=jnp.bfloat16):
    entries = jax.random.normal(key, dims, jnp.float32) * width
    if len(shards) > 0:
        entries = block_levels(key, dims, shards, -0.22, 0.18) * entries
    return jnp.clip(entries, min=-bound, max=bound).astype(kind)


def gaussian_with(rng, dims, scale, reach, cuts, heavy, kind=jnp.bfloat16):
    values = scale * jax.random.normal(rng, dims, jnp.float32)
    if cuts:
        values = values * block_levels(rng, dims, cuts, -0.22, 0.18)
    return jnp.clip(raised(values, jax.random.fold_in(rng, 3), *heavy), -reach, reach).astype(kind)


def setup_inputs(seed: int = 0) -> dict:
    keys = jax.random.split(jax.random.key(seed), 25)
    return {
        "tokens": gaussian(keys[0], (SEQS, D), 1.0, 6.0, ((0, 32),)),
        "mix_gain": jnp.clip(1.0 + 0.18 * jax.random.normal(keys[1], (D,), jnp.float32), 0.1, 1.9),
        "w_query": gaussian(keys[2], (D, HEADS * HD), D ** -0.5, 0.125, ((1, 4),)),
        "w_key": gaussian(keys[3], (D, HEADS * HD), D ** -0.5, 0.125, ((1, 4),)),
        "w_value": gaussian(keys[4], (D, HEADS * HD), D ** -0.5, 0.125, ((1, 4),)),
        "w_outgate": gaussian(keys[5], (D, HEADS * HD), D ** -0.5, 0.125, ((1, 4),)),
        "w_ingate": gaussian(keys[6], (D, HEADS), D ** -0.5, 0.125, ((1, 4),)),
        "w_forget": gaussian(keys[7], (D, HEADS), D ** -0.5, 0.125, ((1, 4),)),
        "in_bias": jnp.clip(-2.0 + 3.0 * jax.random.uniform(keys[8], (HEADS,), jnp.float32) ** block_levels(keys[8], (HEADS,), ((0, 4),), -0.2, 0.2), -2.0, 1.0),
        "forget_bias": jnp.clip(-1.0 + 5.0 * jax.random.uniform(keys[9], (HEADS,), jnp.float32) ** block_levels(keys[9], (HEADS,), ((0, 4),), -0.2, 0.2), -1.0, 4.0),
        "w_mix_out": gaussian(keys[10], (HEADS * HD, D), (HEADS * HD) ** -0.5, 0.1875),
        "cell_state": gaussian(keys[11], (SEQS, HEADS, HD, HD), HD ** -0.5, 0.5, ((0, 32), (1, 4)), jnp.float32),
        "norm_state": gaussian(keys[12], (SEQS, HEADS, HD), HD ** -0.5, 0.5, ((0, 32), (1, 4)), jnp.float32),
        "max_state": jnp.clip(-1.0 + 3.0 * jax.random.uniform(keys[13], (SEQS, HEADS), jnp.float32) ** block_levels(keys[13], (SEQS, HEADS), ((0, 32), (1, 4)), -0.2, 0.2), -1.0, 2.0),
        "moe_gain": jnp.clip(1.0 + 0.18 * jax.random.normal(keys[14], (D,), jnp.float32), 0.1, 1.9),
        "route_ids": draw_route_ids(jax.random.fold_in(keys[24], 71), 0),
        "route_weights": jnp.clip(0.2 + 0.8 * jax.random.uniform(keys[16], (SEQS, TOPK), jnp.float32) ** block_levels(keys[16], (SEQS, TOPK), ((0, 32),), -0.2, 0.2), 0.2, 1.0),
        "expert_gate": gaussian(keys[17], (EXPERTS, D, EXP_FF), D ** -0.5, 0.125, ((0, 32), (2, 4))),
        "expert_up": gaussian(keys[18], (EXPERTS, D, EXP_FF), D ** -0.5, 0.125, ((0, 32), (2, 4))),
        "expert_down": gaussian(keys[19], (EXPERTS, EXP_FF, D), EXP_FF ** -0.5, 0.1875, ((0, 32), (1, 4))),
        "branch_gate": gaussian(keys[20], (D,), D ** -0.5, 0.125),
        "dense_gate": gaussian(keys[21], (D, DFF), D ** -0.5, 0.125, ((1, 128),)),
        "dense_up": gaussian(keys[22], (D, DFF), D ** -0.5, 0.125, ((1, 128),)),
        "dense_down": gaussian_with(keys[23], (DFF, D), DFF ** -0.5, 0.25, ((0, 128),), (0, 1, 128, 5.5)),
    }


EPS = 1e-06

def norm_rows(rows_in, gain_vec):
    as_float = rows_in.astype(jnp.float32)
    scaled = as_float * lax.rsqrt(lax.optimization_barrier(jnp.mean(as_float * as_float, axis=-1, keepdims=True)) + EPS)
    return (scaled * gain_vec).astype(jnp.bfloat16)

def swiglu(tok_rows, gate_w, up_w):
    gate_proj = jnp.dot(tok_rows, gate_w, preferred_element_type=jnp.float32)
    up_proj = jnp.dot(tok_rows, up_w, preferred_element_type=jnp.float32)
    return (jax.nn.silu(gate_proj) * up_proj).astype(jnp.bfloat16)

def cell_step(normed, w_query, w_key, w_value, w_outgate, w_ingate, w_forget, in_bias, forget_bias, cell_state, norm_state, max_state):
    row_count, head_count = max_state.shape
    head_size = cell_state.shape[2]

    def project(weight):
        return jnp.dot(normed, weight, preferred_element_type=jnp.float32)
    queries = project(w_query).reshape(row_count, head_count, head_size)
    key_vecs = project(w_key).reshape(row_count, head_count, head_size) * head_size ** (-0.5)
    values = project(w_value).reshape(row_count, head_count, head_size)
    outgate = project(w_outgate)
    in_pre = project(w_ingate) + in_bias
    log_forget = jax.nn.log_sigmoid(project(w_forget) + forget_bias)
    new_max = jnp.maximum(log_forget + max_state, in_pre)
    carry_factor = jnp.exp(log_forget + max_state - new_max)
    write_factor = jnp.exp(in_pre - new_max)
    written = write_factor[..., None] * key_vecs
    new_cell = carry_factor[..., None, None] * cell_state + written[..., :, None] * values[..., None, :]
    new_norm = carry_factor[..., None] * norm_state + written
    numerator = jnp.einsum('bhd,bhde->bhe', queries, new_cell, precision=lax.Precision.HIGHEST)
    denominator = lax.optimization_barrier(jnp.sum(queries * new_norm, axis=-1))
    cell_out = numerator / jnp.maximum(jnp.abs(denominator), jnp.exp(-new_max))[..., None]
    mixed_heads = (jax.nn.sigmoid(outgate) * cell_out.reshape(row_count, head_count * head_size)).astype(jnp.bfloat16)
    return (mixed_heads, new_cell, new_norm, new_max)

def reference(tokens, mix_gain, w_query, w_key, w_value, w_outgate, w_ingate, w_forget, in_bias, forget_bias, w_mix_out, cell_state, norm_state, max_state, moe_gain, route_ids, route_weights, expert_gate, expert_up, expert_down, branch_gate, dense_gate, dense_up, dense_down):
    normed = norm_rows(tokens, mix_gain)
    mixed_heads, new_cell, new_norm, new_max = cell_step(normed, w_query, w_key, w_value, w_outgate, w_ingate, w_forget, in_bias, forget_bias, cell_state, norm_state, max_state)
    mixed_proj = jnp.dot(mixed_heads, w_mix_out, preferred_element_type=jnp.float32)
    residual = (tokens.astype(jnp.float32) + mixed_proj).astype(jnp.bfloat16)
    moe_in = norm_rows(residual, moe_gain)
    flat_ids = route_ids.reshape(-1)
    owner_row = (jnp.arange(flat_ids.shape[0], dtype=jnp.int32) // route_ids.shape[1]).astype(jnp.int32)
    flat_weights = route_weights.reshape(-1)
    most_rows = N_EP * CAP

    def one_expert(total_out, inputs):
        expert_id, gate_w, up_w, down_w = inputs
        is_routed = flat_ids == expert_id
        slot_index = jnp.cumsum(is_routed.astype(jnp.int32)) - 1
        target = jnp.where(is_routed, slot_index, most_rows).astype(jnp.int32)
        row_index = jnp.zeros((most_rows,), jnp.int32).at[target].set(owner_row, mode='drop')
        slot_weight = jnp.zeros((most_rows,), jnp.float32).at[target].set(flat_weights, mode='drop')
        hidden = swiglu(moe_in[row_index], gate_w, up_w)
        expert_out = jnp.dot(hidden, down_w, preferred_element_type=jnp.float32) * slot_weight[:, None]
        return (total_out.at[row_index].add(expert_out), None)
    moe_out = lax.scan(one_expert, jnp.zeros((SEQS, D), jnp.float32), (jnp.arange(EXPERTS, dtype=jnp.int32), expert_gate, expert_up, expert_down))[0]
    dense_hidden = swiglu(moe_in, dense_gate, dense_up)
    branch_weight = jax.nn.sigmoid(jnp.dot(moe_in, branch_gate, preferred_element_type=jnp.float32))
    dense_out = branch_weight[:, None] * jnp.dot(dense_hidden, dense_down, preferred_element_type=jnp.float32)
    layer_out = (residual.astype(jnp.float32) + moe_out + dense_out).astype(jnp.bfloat16)
    return (layer_out, new_cell, new_norm, new_max)
```

```python
import functools

import jax
import jax.numpy as jnp
from jax import lax
from jax.experimental import pallas as pl
from jax.experimental.pallas import tpu as pltpu
from jax.sharding import PartitionSpec as P

EPS = 1e-06
MESH = pl.DeviceIdType.MESH
F32 = jnp.float32
BF16 = jnp.bfloat16
NT = (((1,), (1,)), ((), ()))


def dot(a, b):
    return jnp.dot(a, b, preferred_element_type=F32)


def dot_nt(a, b):
    return lax.dot_general(a, b, NT, preferred_element_type=F32)


CHUNK = 6
N_CHUNK = 8


def cell_kernel(
    tok_h, gain_h, wq_h, wk_h, wv_h, wo_h, win_h, wf_h, inb, fb, cell_h, norm_h, max_h,
    mixed_o, cell_o, norm_o, max_o,
    tok, gain, wts, win, wf, cell, norm, mx, normed, vs, cb, qt, wt, num,
    wsem, csem, osem, ssem,
):
    small = [
        pltpu.make_async_copy(src, dst, ssem.at[i])
        for i, (src, dst) in enumerate(
            [(tok_h, tok), (gain_h, gain), (win_h, win), (wf_h, wf), (norm_h, norm), (max_h, mx)]
        )
    ]
    for cp in small:
        cp.start()
    wcp = [pltpu.make_async_copy(src, wts.at[i], wsem.at[i]) for i, src in enumerate([wq_h, wk_h, wv_h, wo_h])]
    for cp in wcp:
        cp.start()

    def cin(i):
        s = pl.ds(i * CHUNK, CHUNK)
        return pltpu.make_async_copy(cell_h.at[s], cell.at[s], csem.at[i])

    def cout(i):
        s = pl.ds(i * CHUNK, CHUNK)
        return pltpu.make_async_copy(cell.at[s], cell_o.at[s], osem.at[i])

    for i in range(N_CHUNK):
        cin(i).start()
    for cp in small:
        cp.wait()

    xf = tok[...].astype(F32)
    ms = jnp.mean(xf * xf, axis=-1, keepdims=True)
    normed[...] = (xf * lax.rsqrt(ms + EPS) * gain[...]).astype(BF16)
    nb = normed[...]
    in_pre = dot_nt(win[...], nb)
    fpre = dot_nt(wf[...], nb)
    hrow = lax.broadcasted_iota(jnp.int32, in_pre.shape, 0)
    in_pre = in_pre + jnp.where(hrow == 0, inb[0], inb[1])
    fpre = fpre + jnp.where(hrow == 0, fb[0], fb[1])
    log_f = jnp.minimum(fpre, 0.0) - jnp.log1p(jnp.exp(-jnp.abs(fpre)))
    lm = log_f + mx[...]
    new_max = jnp.maximum(lm, in_pre)
    max_o[...] = new_max
    carry = jnp.exp(lm - new_max)
    write = jnp.exp(in_pre - new_max)
    floor = jnp.exp(-new_max)
    rows = jnp.concatenate([carry, write, floor], axis=0)
    rows = jnp.concatenate([rows, jnp.zeros((6, 80), F32)], axis=1)
    rows = jnp.concatenate([rows, jnp.zeros((122, 128), F32)], axis=0)
    cols = rows.T

    wcp[0].wait()
    q = dot(nb, wts[0])
    wcp[1].wait()
    k = dot(nb, wts[1]) * (128 ** (-0.5))
    wcp[2].wait()
    v = dot(nb, wts[2])
    vs[0] = v[:, 0:128]
    vs[1] = v[:, 128:256]
    wcp[3].wait()
    og = jax.nn.sigmoid(dot(nb, wts[3]))

    denom = []
    pad = jnp.zeros((80, 128), F32)
    for h in range(2):
        ca = jnp.broadcast_to(cols[0:48, h : h + 1], (48, 128))
        wr = jnp.broadcast_to(cols[0:48, 2 + h : 3 + h], (48, 128))
        qh = q[:, h * 128 : (h + 1) * 128]
        written = wr * k[:, h * 128 : (h + 1) * 128]
        hs = pl.ds(h, 48, stride=2)
        nn = ca * norm[hs, :] + written
        norm_o[hs, :] = nn
        den = jnp.sum(qh * nn, axis=-1, keepdims=True)
        denom.append(jnp.maximum(jnp.abs(den), cols[0:48, 4 + h : 5 + h]))
        cb[h] = ca
        qt[h] = jnp.concatenate([qh, pad], axis=0).T
        wt[h] = jnp.concatenate([written, pad], axis=0).T

    def step(i, _):
        cin(i).wait()
        shift = lax.rem(128 - i * CHUNK, 128)
        for h in range(2):
            qi = pltpu.roll(qt[h], shift, 1)
            wi = pltpu.roll(wt[h], shift, 1)
            for j in range(CHUNK):
                b = i * CHUNK + j
                row = pl.ds(b, 1)
                new = cb[h, row, :] * cell[b, h] + wi[:, j : j + 1] * vs[h, row, :]
                cell[b, h] = new
                num[h, row, :] = jnp.sum(qi[:, j : j + 1] * new, axis=0, keepdims=True)
        cout(i).start()
        return 0

    lax.fori_loop(0, N_CHUNK, step, 0)
    for h in range(2):
        lanes = slice(h * 128, (h + 1) * 128)
        mixed_o[:, lanes] = (og[:, lanes] * (num[h] / denom[h])).astype(BF16)
    for i in range(N_CHUNK):
        cout(i).wait()


def cell_call(*args):
    any_ = pl.BlockSpec(memory_space=pl.ANY)
    vm = pl.BlockSpec(memory_space=pltpu.VMEM)
    sm = pl.BlockSpec(memory_space=pltpu.SMEM)
    return pl.pallas_call(
        cell_kernel,
        out_shape=(
            jax.ShapeDtypeStruct((48, 256), BF16),
            jax.ShapeDtypeStruct((48, 2, 128, 128), F32),
            jax.ShapeDtypeStruct((96, 128), F32),
            jax.ShapeDtypeStruct((2, 48), F32),
        ),
        in_specs=[any_] * 8 + [sm, sm] + [any_] * 3,
        out_specs=(vm, any_, vm, vm),
        scratch_shapes=[
            pltpu.VMEM((48, 2048), BF16),
            pltpu.VMEM((1, 2048), F32),
            pltpu.VMEM((4, 2048, 256), BF16),
            pltpu.VMEM((2, 2048), BF16),
            pltpu.VMEM((2, 2048), BF16),
            pltpu.VMEM((48, 2, 128, 128), F32),
            pltpu.VMEM((96, 128), F32),
            pltpu.VMEM((2, 48), F32),
            pltpu.VMEM((48, 2048), BF16),
            pltpu.VMEM((2, 48, 128), F32),
            pltpu.VMEM((2, 48, 128), F32),
            pltpu.VMEM((2, 128, 128), F32),
            pltpu.VMEM((2, 128, 128), F32),
            pltpu.VMEM((2, 48, 128), F32),
            pltpu.SemaphoreType.DMA((4,)),
            pltpu.SemaphoreType.DMA((N_CHUNK,)),
            pltpu.SemaphoreType.DMA((N_CHUNK,)),
            pltpu.SemaphoreType.DMA((6,)),
        ],
        compiler_params=pltpu.CompilerParams(vmem_limit_bytes=20 * 2**20),
        name="cell",
    )(*args)


REL = [
    (0, 0), (1, 0), (3, 0), (0, 1), (0, 3),
    (1, 1), (1, 3), (3, 1), (3, 3), (2, 0), (0, 2),
    (2, 1), (2, 3), (1, 2), (3, 2),
    (2, 2),
]
IDX = {rel: i for i, rel in enumerate(REL)}
GROUPS = [(0, 5), (5, 6), (11, 4), (15, 1)]
ZP, ZM, YP, YM = (1, 0), (3, 0), (0, 1), (0, 3)
N_MSG = 160


def layer_kernel(
    mixed_h, tok_h, wmix_h, gain_h, bg_h, ids_h, rw_h, gate_h, up_h, down_h, eg_h, eu_h, ed_h,
    out,
    ah, tok, wmix, gain, bg, ids, rw, w, d, eg, eu, ed, meta, g, res, hid, xo, xp, xb, xs, eh, sb, rsr, rb, eret,
    ssem, rsem, lsem,
):
    me = lax.axis_index("ep")
    x = lax.axis_index("tp")
    c = lax.rem(me, 2)
    zy = lax.div(me, 2)
    y = lax.rem(zy, 4)
    z = lax.div(zy, 4)

    def dev(dz, dy, dx, pc):
        zz = lax.rem(z + dz, 4)
        yy = lax.rem(y + dy, 4)
        cc = 1 - c if pc else c
        return ((zz * 4 + yy) * 2 + cc, lax.rem(x + dx, 4))

    count = [0]
    sent = []

    class Msg:
        def __init__(self, src, dst, device, land=None):
            n = count[0]
            count[0] += 1
            self.copy = pltpu.make_async_remote_copy(
                src_ref=src, dst_ref=dst, send_sem=ssem.at[n], recv_sem=rsem.at[n], device_id=device, device_id_type=MESH
            )

        def start(self):
            self.copy.start()
            sent.append(self.copy)
            return self

        def arrived(self):
            self.copy.wait_recv()

    local = []

    def load(src, dst):
        cp = pltpu.make_async_copy(src, dst, lsem.at[len(local)])
        local.append(cp)
        cp.start()
        return cp

    barrier = pltpu.get_barrier_semaphore()
    peers = [dev(0, 0, 1, 0), dev(0, 0, 2, 0), dev(0, 0, 3, 0), dev(0, 0, 0, 1)]
    peers += [dev(dz, dy, 0, 0) for dz, dy in (ZP, ZM, YP, YM)]
    for peer in peers:
        pl.semaphore_signal(barrier, inc=1, device_id=peer, device_id_type=MESH)

    mine = pl.ds(pl.multiple_of(x * 256, 256), 256)
    cp_mixed = load(mixed_h, ah.at[:, mine])
    cp_ids = load(ids_h, ids)
    cp_rw = load(rw_h, rw)
    cp_tok = load(tok_h, tok)
    cp_gain = load(gain_h, gain)
    cp_bg = load(bg_h, bg)
    cp_wmix = load(wmix_h, wmix)
    cp_gate = load(gate_h, w.at[0:64])
    cp_up = load(up_h, w.at[128:192])
    cols = pl.ds(pl.multiple_of(x * 512, 512), 512)
    cp_down = load(down_h.at[:, cols], d.at[0:64])
    cp_ed = load(ed_h.at[:, cols], ed.at[0:256])
    cp_eg = load(eg_h, eg)
    cp_eu = load(eu_h, eu)

    cp_ids.wait()
    cp_rw.wait()
    idf = ids[...].astype(F32)
    four = jnp.concatenate([idf, rw[...]], axis=0)
    four = jnp.concatenate([four, jnp.zeros((4, 80), F32)], axis=1)
    four = jnp.concatenate([four, jnp.zeros((124, 128), F32)], axis=0)
    idc = four.T
    before = lax.broadcasted_iota(jnp.int32, (48, 48), 0) < lax.broadcasted_iota(jnp.int32, (48, 48), 1)
    slots = []
    for ch in range(2):
        row = idf[ch : ch + 1, :]
        hits = jnp.where(idc[0:48, 0:1] == row, 1.0, 0.0) + jnp.where(idc[0:48, 1:2] == row, 1.0, 0.0)
        rank = jnp.sum(jnp.where(before, hits, 0.0), axis=0, keepdims=True)
        slots.append(row * 16.0 + rank)
    srow = jnp.concatenate(slots + [jnp.zeros((6, 48), F32)], axis=0)
    srow = jnp.concatenate([srow, jnp.zeros((8, 80), F32)], axis=1)
    meta[zy] = srow
    scol = jnp.concatenate([srow, jnp.zeros((120, 128), F32)], axis=0).T

    pl.semaphore_wait(barrier, len(peers))

    cp_mixed.wait()
    heads = [Msg(ah.at[:, mine], ah.at[:, mine], dev(0, 0, dx, 0)).start() for dx in (1, 3, 2)]
    m_z = [Msg(meta.at[zy], meta.at[zy], dev(*k, 0, 0)).start() for k in (ZP, ZM)]
    w_p = [
        Msg(gate_h, w.at[64:128], dev(0, 0, 0, 1)).start(),
        Msg(up_h, w.at[192:256], dev(0, 0, 0, 1)).start(),
    ]
    down_x, ed_x = {}, {}
    for dx in (1, 3, 2):
        their = pl.ds(pl.multiple_of(lax.rem(x + dx, 4) * 512, 512), 512)
        s = (4 - dx) % 4
        down_x[s] = Msg(down_h.at[:, their], d.at[s * 128 : s * 128 + 64], dev(0, 0, dx, 0)).start()
        ed_x[s] = Msg(ed_h.at[:, their], ed.at[s * 256 : s * 256 + 256], dev(0, 0, dx, 0)).start()
    down_p = [Msg(down_h.at[:, cols], d.at[64:128], dev(0, 0, 0, 1)).start()]

    cp_wmix.wait()
    cp_tok.wait()
    cp_gain.wait()
    cp_bg.wait()
    for m in heads:
        m.arrived()

    sq = jnp.zeros((48, 1), F32)
    for n in range(4):
        s = slice(n * 512, (n + 1) * 512)
        r = (tok[:, s].astype(F32) + dot(ah[...], wmix[:, s])).astype(BF16)
        res[:, s] = r
        rf = r.astype(F32)
        sq = sq + jnp.sum(rf * rf, axis=-1, keepdims=True)
    inv = lax.rsqrt(sq * (1.0 / 2048.0) + EPS)
    gate_sum = jnp.zeros((48, 1), F32)
    for n in range(4):
        s = slice(n * 512, (n + 1) * 512)
        mi = (res[:, s].astype(F32) * inv * gain[:, s]).astype(BF16)
        g[0, n] = mi
        gate_sum = gate_sum + jnp.sum(mi.astype(F32) * bg[:, s].astype(F32), axis=-1, keepdims=True)
    bw = jax.nn.sigmoid(gate_sum)

    def spread(rel, q0, nq, way):
        to = ((rel[0] - way[0]) % 4, (rel[1] - way[1]) % 4)
        q = pl.ds(q0, nq)
        return Msg(g.at[IDX[rel], q], g.at[IDX[to], q], dev(*way, 0, 0)).start()

    O = (0, 0)
    a_zp, a_zm = spread(O, 0, 2, ZP), spread(O, 0, 2, ZM)
    b_yp, b_ym = spread(O, 2, 2, YP), spread(O, 2, 2, YM)
    a_yp, a_ym = spread(O, 0, 2, YP), spread(O, 0, 2, YM)
    b_zp, b_zm = spread(O, 2, 2, ZP), spread(O, 2, 2, ZM)

    for m in m_z:
        m.arrived()
    zmy = lax.rem(z + 3, 4) * 4 + y
    m_z2 = Msg(meta.at[zmy], meta.at[zmy], dev(*ZP, 0, 0)).start()

    a_zp.arrived()
    f_z0 = spread((3, 0), 0, 1, ZP)
    t_33, t_31 = spread((3, 0), 0, 2, YP), spread((3, 0), 0, 2, YM)
    a_zm.arrived()
    f_z1 = spread((1, 0), 1, 1, ZM)
    t_13, t_11 = spread((1, 0), 0, 2, YP), spread((1, 0), 0, 2, YM)
    b_yp.arrived()
    f_y2 = spread((0, 3), 2, 1, YP)
    u_33, u_13 = spread((0, 3), 2, 2, ZP), spread((0, 3), 2, 2, ZM)
    b_ym.arrived()
    f_y3 = spread((0, 1), 3, 1, YM)
    u_31, u_11 = spread((0, 1), 2, 2, ZP), spread((0, 1), 2, 2, ZM)
    a_yp.arrived()
    f_y0 = spread((0, 3), 0, 1, YP)
    a_ym.arrived()
    f_y1 = spread((0, 1), 1, 1, YM)
    b_zp.arrived()
    f_z2 = spread((3, 0), 2, 1, ZP)
    b_zm.arrived()
    f_z3 = spread((1, 0), 3, 1, ZM)

    m_z2.arrived()
    m_y = []
    for k in (YP, YM):
        for zz in range(4):
            m_y.append(Msg(meta.at[zz * 4 + y], meta.at[zz * 4 + y], dev(*k, 0, 0)).start())

    cp_gate.wait()
    cp_up.wait()
    for m in w_p:
        m.arrived()
    cp_down.wait()
    for s in (1, 2, 3):
        down_x[s].arrived()
        own = slice(s * 128, s * 128 + 64)
        down_p.append(Msg(d.at[own], d.at[s * 128 + 64 : s * 128 + 128], dev(0, 0, 0, 1)).start())

    def up_group(n):
        r0, nb = GROUPS[n]
        acc = None
        for q in range(4):
            part = dot_nt(g[r0 : r0 + nb, q].reshape(nb * 48, 512), w[:, q * 512 : (q + 1) * 512])
            acc = part if acc is None else acc + part
        ga, up = acc[:, 0:128], acc[:, 128:256]
        rows = pl.ds(r0 * 48, nb * 48)
        hid[rows, 0:128] = (ga * jax.nn.sigmoid(ga) * up).astype(BF16)
        out = {}
        for dx in (1, 3, 2):
            s = (4 - dx) % 4
            out[s] = Msg(hid.at[rows, 0:128], hid.at[rows, s * 128 : s * 128 + 128], dev(0, 0, dx, 0)).start()
        return out

    e_mine = (me * 16).astype(F32)
    e_other = ((zy * 2 + (1 - c)) * 16).astype(F32)

    def pick_group(n):
        r0, nb = GROUPS[n]
        lane8 = lax.broadcasted_iota(jnp.int32, (8, 48), 0).astype(F32)
        code = jnp.concatenate([lane8 + e_mine, lane8 + e_other], axis=0)
        for r in range(r0, r0 + nb):
            dz, dy = REL[r]
            owner = lax.rem(z + dz, 4) * 4 + lax.rem(y + dy, 4)
            m = meta[owner]
            hit = jnp.where(m[0:1, 0:48] == code, 1.0, 0.0) + jnp.where(m[1:2, 0:48] == code, 1.0, 0.0)
            hit = hit.astype(BF16)
            for q in range(4):
                picked = dot(hit, g[r, q])
                s = slice(q * 512, (q + 1) * 512)
                xo[r * 8 : r * 8 + 8, s] = picked[0:8]
                xp[r * 8 : r * 8 + 8, s] = picked[8:16]

    def pass_rows(a, b):
        rows = slice(a, b)
        xs[rows] = xp[rows].astype(BF16)
        return Msg(xs.at[rows], xb.at[rows], dev(0, 0, 0, 1)).start()

    f_z0.arrived()
    f_z1.arrived()
    t_23, t_21 = spread((2, 0), 0, 2, YP), spread((2, 0), 0, 2, YM)
    f_y2.arrived()
    f_y3.arrived()
    u_32, u_12 = spread((0, 2), 2, 2, ZP), spread((0, 2), 2, 2, ZM)
    t_33.arrived()
    h_32a = spread((3, 3), 0, 1, YP)
    t_31.arrived()
    h_32b = spread((3, 1), 1, 1, YM)
    t_13.arrived()
    h_12a = spread((1, 3), 0, 1, YP)
    t_11.arrived()
    h_12b = spread((1, 1), 1, 1, YM)
    u_33.arrived()
    h_23a = spread((3, 3), 2, 1, ZP)
    u_13.arrived()
    h_23b = spread((1, 3), 3, 1, ZM)
    u_31.arrived()
    h_21a = spread((3, 1), 2, 1, ZP)
    u_11.arrived()
    h_21b = spread((1, 1), 3, 1, ZM)

    for m in m_y:
        m.arrived()
    m_y2 = []
    ym = lax.rem(y + 3, 4)
    for zz in range(4):
        m_y2.append(Msg(meta.at[zz * 4 + ym], meta.at[zz * 4 + ym], dev(*YP, 0, 0)).start())

    hid_in = {}
    hid_in[0] = up_group(0)
    pick_group(0)
    for m in (f_y0, f_y1, f_z2, f_z3):
        m.arrived()
    for m in m_y2:
        m.arrived()

    t_23.arrived()
    l_22a = spread((2, 3), 0, 1, YP)
    t_21.arrived()
    l_22b = spread((2, 1), 1, 1, YM)
    u_32.arrived()
    l_22c = spread((3, 2), 2, 1, ZP)
    u_12.arrived()
    l_22d = spread((1, 2), 3, 1, ZM)

    hid_in[1] = up_group(1)
    pick_group(1)

    for m in down_p:
        m.arrived()

    reduced = []

    def down_group(n):
        r0, nb = GROUPS[n]
        for m in hid_in[n].values():
            m.arrived()
        part = dot(hid[r0 * 48 : (r0 + nb) * 48, :], d[...])
        for i in range(nb):
            r = r0 + i
            blk = part[i * 48 : (i + 1) * 48].astype(BF16)
            if r == 0:
                rsr[0] = blk
            else:
                dz, dy = REL[r]
                sb[r] = blk
                back = IDX[((-dz) % 4, (-dy) % 4)]
                reduced.append(Msg(sb.at[r], rsr.at[back], dev(dz, dy, 0, 0)).start())

    for m in (h_32a, h_32b, h_12a, h_12b, h_23a, h_23b, h_21a, h_21b):
        m.arrived()
    hid_in[2] = up_group(2)
    pick_group(2)
    passed = [pass_rows(0, 112)]
    down_group(0)
    for m in (l_22a, l_22b, l_22c, l_22d):
        m.arrived()
    hid_in[3] = up_group(3)
    pick_group(3)
    passed.append(pass_rows(112, 128))

    cp_eg.wait()
    cp_eu.wait()

    def expert_up(half, rows_in):
        ga = dot(rows_in, eg[...])
        up = dot(rows_in, eu[...])
        eh[half, :, 0:256] = (ga * jax.nn.sigmoid(ga) * up).astype(BF16)
        out = []
        for dx in (1, 3, 2):
            s = (4 - dx) % 4
            out.append(Msg(eh.at[half, :, 0:256], eh.at[half, :, s * 256 : s * 256 + 256], dev(0, 0, dx, 0)).start())
        return out

    eh_in = [expert_up(0, xo[...].astype(BF16))]
    for m in passed:
        m.arrived()
    eh_in.append(expert_up(1, xb[...]))

    down_group(1)
    down_group(2)
    down_group(3)

    cp_ed.wait()
    for m in ed_x.values():
        m.arrived()
    returned = []
    for half in range(2):
        for m in eh_in[half]:
            m.arrived()
        eo = dot(eh[half], ed[...])
        for r in range(16):
            rows = slice(r * 8, r * 8 + 8)
            blk = jnp.concatenate([eo[rows, 0:256], eo[rows, 256:512]], axis=0).astype(BF16)
            if r == 0 and half == 0:
                eret[me] = blk
            else:
                dz, dy = REL[r]
                rb[half, r] = blk
                returned.append(Msg(rb.at[half, r], eret.at[me], dev(dz, dy, 0, half)).start())

    total = rsr[0].astype(F32)
    for m in reduced:
        m.arrived()
    for r in range(1, 16):
        total = total + rsr[r].astype(F32)
    own_res = res[:, cols].astype(F32)
    for m in returned:
        m.arrived()
    back = eret[...].reshape(512, 256)
    lane = lax.broadcasted_iota(jnp.int32, (48, 512), 1).astype(F32)
    for hf in range(2):
        s = slice(hf * 256, hf * 256 + 256)
        moe = jnp.zeros((48, 256), F32)
        for ch in range(2):
            want = scol[0:48, ch : ch + 1] + float(hf * 8)
            sel = jnp.where(lane == want, 1.0, 0.0).astype(BF16)
            moe = moe + dot(sel, back) * idc[0:48, 2 + ch : 3 + ch]
        out[:, s] = (own_res[:, s] + moe + bw * total[:, s]).astype(BF16)

    for cp in sent:
        cp.wait_send()


def layer_call(*args):
    any_ = pl.BlockSpec(memory_space=pl.ANY)
    vm = pl.BlockSpec(memory_space=pltpu.VMEM)
    return pl.pallas_call(
        layer_kernel,
        out_shape=jax.ShapeDtypeStruct((48, 512), BF16),
        in_specs=[any_] * 13,
        out_specs=vm,
        scratch_shapes=[
            pltpu.VMEM((48, 1024), BF16),
            pltpu.VMEM((48, 2048), BF16),
            pltpu.VMEM((1024, 2048), BF16),
            pltpu.VMEM((1, 2048), F32),
            pltpu.VMEM((1, 2048), BF16),
            pltpu.VMEM((2, 48), jnp.int32),
            pltpu.VMEM((2, 48), F32),
            pltpu.VMEM((256, 2048), BF16),
            pltpu.VMEM((512, 512), BF16),
            pltpu.VMEM((2048, 256), BF16),
            pltpu.VMEM((2048, 256), BF16),
            pltpu.VMEM((1024, 512), BF16),
            pltpu.VMEM((16, 8, 128), F32),
            pltpu.VMEM((16, 4, 48, 512), BF16),
            pltpu.VMEM((48, 2048), BF16),
            pltpu.VMEM((768, 512), BF16),
            pltpu.VMEM((128, 2048), F32),
            pltpu.VMEM((128, 2048), F32),
            pltpu.VMEM((128, 2048), BF16),
            pltpu.VMEM((128, 2048), BF16),
            pltpu.VMEM((2, 128, 1024), BF16),
            pltpu.VMEM((16, 48, 512), BF16),
            pltpu.VMEM((16, 48, 512), BF16),
            pltpu.VMEM((2, 16, 16, 256), BF16),
            pltpu.VMEM((32, 16, 256), BF16),
            pltpu.SemaphoreType.DMA((N_MSG,)),
            pltpu.SemaphoreType.DMA((N_MSG,)),
            pltpu.SemaphoreType.DMA((16,)),
        ],
        compiler_params=pltpu.CompilerParams(vmem_limit_bytes=36 * 2**20, collective_id=0, has_side_effects=True),
        name="layer",
    )(*args)


def local(
    tokens, mix_gain, w_query, w_key, w_value, w_outgate, w_ingate, w_forget, in_bias, forget_bias, w_mix_out,
    cell_state, norm_state, max_state, moe_gain, route_ids, route_weights, expert_gate, expert_up, expert_down,
    branch_gate, dense_gate, dense_up, dense_down,
):
    mixed, new_cell, new_norm, new_max = cell_call(
        tokens, mix_gain.reshape(1, 2048), w_query, w_key, w_value, w_outgate, w_ingate.T, w_forget.T,
        in_bias, forget_bias, cell_state, norm_state.reshape(96, 128), max_state.T,
    )
    layer_out = layer_call(
        mixed, tokens, w_mix_out, moe_gain.reshape(1, 2048), branch_gate.reshape(1, 2048), route_ids.T, route_weights.T,
        dense_gate.T, dense_up.T, dense_down,
        expert_gate.reshape(2048, 256), expert_up.reshape(2048, 256), expert_down.reshape(256, 2048),
    )
    return (layer_out, new_cell, new_norm.reshape(48, 2, 128), new_max.T)


def solution(mesh):
    in_specs = (
        P("ep", None),
        P(),
        P(None, "tp"),
        P(None, "tp"),
        P(None, "tp"),
        P(None, "tp"),
        P(None, "tp"),
        P(None, "tp"),
        P("tp"),
        P("tp"),
        P(),
        P("ep", "tp", None, None),
        P("ep", "tp", None),
        P("ep", "tp"),
        P(),
        P("ep", None),
        P("ep", None),
        P("ep", None, "tp"),
        P("ep", None, "tp"),
        P("ep", "tp", None),
        P(),
        P(None, ("ep", "tp")),
        P(None, ("ep", "tp")),
        P(("ep", "tp"), None),
    )
    out_specs = (P("ep", "tp"), P("ep", "tp", None, None), P("ep", "tp", None), P("ep", "tp"))
    return jax.shard_map(local, mesh=mesh, in_specs=in_specs, out_specs=out_specs, check_vma=False)
```

```python
import functools

import jax
import jax.numpy as jnp
from jax import lax
from jax.experimental import pallas as pl
from jax.experimental.pallas import tpu as pltpu
from jax.sharding import PartitionSpec as P

EPS = 1e-06
MESH = pl.DeviceIdType.MESH
F32 = jnp.float32
BF16 = jnp.bfloat16
NT = (((1,), (1,)), ((), ()))


def dot(a, b):
    return jnp.dot(a, b, preferred_element_type=F32)


def dot_nt(a, b):
    return lax.dot_general(a, b, NT, preferred_element_type=F32)


CHUNK = 6
N_CHUNK = 8


def split3(a):
    first = a.astype(BF16).astype(F32)
    rest = a - first
    second = rest.astype(BF16).astype(F32)
    return first, second, rest - second


def as_columns(rows):
    n, width = rows.shape
    wide = jnp.concatenate([rows, jnp.zeros((n, 128 - width), F32)], axis=1) if width < 128 else rows
    return jnp.concatenate([wide, jnp.zeros((128 - n, 128), F32)], axis=0).T


def slot_rows(ids):
    idf = ids.astype(F32)
    idc = as_columns(idf)
    before = lax.broadcasted_iota(jnp.int32, (48, 48), 0) < lax.broadcasted_iota(jnp.int32, (48, 48), 1)
    slots = []
    for ch in range(2):
        row = idf[ch : ch + 1, :]
        hits = jnp.where(idc[0:48, 0:1] == row, 1.0, 0.0) + jnp.where(idc[0:48, 1:2] == row, 1.0, 0.0)
        rank = jnp.sum(jnp.where(before, hits, 0.0), axis=0, keepdims=True)
        slots.append(row * 16.0 + rank)
    srow = jnp.concatenate(slots + [jnp.zeros((6, 48), F32)], axis=0)
    return jnp.concatenate([srow, jnp.zeros((8, 80), F32)], axis=1)


def cell_kernel(
    tok_h, gain_h, wq_h, wk_h, wv_h, wo_h, win_h, wf_h, inb, fb, cell_h, norm_h, max_h, ids_h,
    mixed_o, cell_o, norm_o, max_o, slot_o,
    tok, gain, wts, win, wf, cell, norm, mx, ids, normed, vs, cb, qt, wt, num,
    wsem, csem, osem, ssem,
):
    small = [
        pltpu.make_async_copy(src, dst, ssem.at[i])
        for i, (src, dst) in enumerate(
            [(tok_h, tok), (gain_h, gain), (win_h, win), (wf_h, wf), (norm_h, norm), (max_h, mx), (ids_h, ids)]
        )
    ]
    for cp in small:
        cp.start()
    wcp = [pltpu.make_async_copy(src, wts.at[i], wsem.at[i]) for i, src in enumerate([wq_h, wk_h, wv_h, wo_h])]
    for cp in wcp:
        cp.start()

    def cin(i):
        s = pl.ds(i * CHUNK, CHUNK)
        return pltpu.make_async_copy(cell_h.at[s], cell.at[s], csem.at[i])

    def cout(i):
        s = pl.ds(i * CHUNK, CHUNK)
        return pltpu.make_async_copy(cell.at[s], cell_o.at[s], osem.at[i])

    for cp in small:
        cp.wait()
    slot_o[...] = slot_rows(ids[...])

    xf = tok[...].astype(F32)
    ms = jnp.mean(xf * xf, axis=-1, keepdims=True)
    normed[...] = (xf * lax.rsqrt(ms + EPS) * gain[...]).astype(BF16)
    nb = normed[...]
    in_pre = dot_nt(win[...], nb)
    fpre = dot_nt(wf[...], nb)
    hrow = lax.broadcasted_iota(jnp.int32, in_pre.shape, 0)
    in_pre = in_pre + jnp.where(hrow == 0, inb[0], inb[1])
    fpre = fpre + jnp.where(hrow == 0, fb[0], fb[1])
    log_f = jnp.minimum(fpre, 0.0) - jnp.log1p(jnp.exp(-jnp.abs(fpre)))
    lm = log_f + mx[...]
    new_max = jnp.maximum(lm, in_pre)
    max_o[...] = new_max
    carry = jnp.exp(lm - new_max)
    write = jnp.exp(in_pre - new_max)
    floor = jnp.exp(-new_max)
    rows = jnp.concatenate([carry, write, floor], axis=0)
    rows = jnp.concatenate([rows, jnp.zeros((6, 80), F32)], axis=1)
    rows = jnp.concatenate([rows, jnp.zeros((122, 128), F32)], axis=0)
    cols = rows.T

    wcp[0].wait()
    for i in range(2):
        cin(i).start()
    q = dot(nb, wts[0])
    wcp[1].wait()
    for i in range(2, 5):
        cin(i).start()
    k = dot(nb, wts[1]) * (128 ** (-0.5))
    wcp[2].wait()
    for i in range(5, N_CHUNK):
        cin(i).start()
    v = dot(nb, wts[2])
    for h in range(2):
        v1, v2, _ = split3(v[:, h * 128 : (h + 1) * 128])
        vs[h] = jnp.concatenate([v1, v1, v2], axis=0).astype(BF16)
    wcp[3].wait()
    og = jax.nn.sigmoid(dot(nb, wts[3]))

    denom = []
    pad = jnp.zeros((112, 128), F32)
    for h in range(2):
        ca = jnp.broadcast_to(cols[0:48, h : h + 1], (48, 128))
        wr = jnp.broadcast_to(cols[0:48, 2 + h : 3 + h], (48, 128))
        qh = q[:, h * 128 : (h + 1) * 128]
        written = wr * k[:, h * 128 : (h + 1) * 128]
        hs = pl.ds(h, 48, stride=2)
        nn = ca * norm[hs, :] + written
        norm_o[hs, :] = nn
        den = jnp.sum(qh * nn, axis=-1, keepdims=True)
        denom.append(jnp.maximum(jnp.abs(den), cols[0:48, 4 + h : 5 + h]))
        cb[h] = ca
        q1, q2, q3 = split3(qh)
        qt[h] = jnp.concatenate([q1, q2, q3, pad], axis=0).T[:, 0:144].astype(BF16)
        w1, w2, _ = split3(written)
        wt[h] = jnp.concatenate([w1, w2, w1, pad], axis=0).T[:, 0:144].astype(BF16)

    token = lax.rem(lax.broadcasted_iota(jnp.int32, (144, 128), 0), 48)

    def step(i, _):
        cin(i).wait()
        here = [token == i * CHUNK + j for j in range(CHUNK)]
        ones = jnp.concatenate([jnp.where(m, 1.0, 0.0) for m in here], axis=1).astype(BF16)
        for h in range(2):
            vh = vs[h].astype(F32)
            vrows = jnp.concatenate([jnp.where(m, vh, 0.0) for m in here], axis=1).astype(BF16)
            outer = dot(wt[h], vrows)
            qcols = dot(qt[h], ones)
            for j in range(CHUNK):
                b = i * CHUNK + j
                row = pl.ds(b, 1)
                lanes = slice(j * 128, (j + 1) * 128)
                new = cb[h, row, :] * cell[b, h] + outer[:, lanes]
                cell[b, h] = new
                num[h, row, :] = jnp.sum(qcols[:, lanes] * new, axis=0, keepdims=True)
        cout(i).start()
        return 0

    lax.fori_loop(0, N_CHUNK, step, 0)
    for h in range(2):
        lanes = slice(h * 128, (h + 1) * 128)
        mixed_o[:, lanes] = (og[:, lanes] * (num[h] / denom[h])).astype(BF16)
    for i in range(N_CHUNK):
        cout(i).wait()


def cell_call(*args):
    any_ = pl.BlockSpec(memory_space=pl.ANY)
    vm = pl.BlockSpec(memory_space=pltpu.VMEM)
    sm = pl.BlockSpec(memory_space=pltpu.SMEM)
    return pl.pallas_call(
        cell_kernel,
        out_shape=(
            jax.ShapeDtypeStruct((48, 256), BF16),
            jax.ShapeDtypeStruct((48, 2, 128, 128), F32),
            jax.ShapeDtypeStruct((96, 128), F32),
            jax.ShapeDtypeStruct((2, 48), F32),
            jax.ShapeDtypeStruct((8, 128), F32),
        ),
        in_specs=[any_] * 8 + [sm, sm] + [any_] * 4,
        out_specs=(vm, any_, vm, vm, vm),
        scratch_shapes=[
            pltpu.VMEM((48, 2048), BF16),
            pltpu.VMEM((1, 2048), F32),
            pltpu.VMEM((4, 2048, 256), BF16),
            pltpu.VMEM((2, 2048), BF16),
            pltpu.VMEM((2, 2048), BF16),
            pltpu.VMEM((48, 2, 128, 128), F32),
            pltpu.VMEM((96, 128), F32),
            pltpu.VMEM((2, 48), F32),
            pltpu.VMEM((2, 48), jnp.int32),
            pltpu.VMEM((48, 2048), BF16),
            pltpu.VMEM((2, 144, 128), BF16),
            pltpu.VMEM((2, 48, 128), F32),
            pltpu.VMEM((2, 128, 144), BF16),
            pltpu.VMEM((2, 128, 144), BF16),
            pltpu.VMEM((2, 48, 128), F32),
            pltpu.SemaphoreType.DMA((4,)),
            pltpu.SemaphoreType.DMA((N_CHUNK,)),
            pltpu.SemaphoreType.DMA((N_CHUNK,)),
            pltpu.SemaphoreType.DMA((7,)),
        ],
        compiler_params=pltpu.CompilerParams(vmem_limit_bytes=67043328),
        name="cell",
    )(*args)


REL = [
    (0, 0), (1, 0), (3, 0), (0, 1), (0, 3),
    (1, 1), (1, 3), (3, 1), (3, 3), (2, 0), (0, 2),
    (2, 1), (2, 3), (1, 2), (3, 2),
    (2, 2),
]
IDX = {rel: i for i, rel in enumerate(REL)}
GROUPS = [(0, 5), (5, 6), (11, 4), (15, 1)]
ZP, ZM, YP, YM = (1, 0), (3, 0), (0, 1), (0, 3)
N_MSG = 160


def layer_kernel(
    mixed_h, tok_h, wmix_h, gain_h, bg_h, slot_h, rw_h, gate_h, up_h, down_h, eg_h, eu_h, ed_h,
    out,
    ah, tok, wmix, gain, bg, macc, rw, w, d, eg, eu, ed, meta, g, res, hid, xo, xp, xb, xs, eh, el, sb, rsr, rb, eret,
    ssem, rsem, lsem,
):
    me = lax.axis_index("ep")
    x = lax.axis_index("tp")
    c = lax.rem(me, 2)
    zy = lax.div(me, 2)
    y = lax.rem(zy, 4)
    z = lax.div(zy, 4)

    def dev(dz, dy, dx, pc):
        zz = lax.rem(z + dz, 4)
        yy = lax.rem(y + dy, 4)
        cc = 1 - c if pc else c
        return ((zz * 4 + yy) * 2 + cc, lax.rem(x + dx, 4))

    count = [0]
    sent = []

    class Msg:
        def __init__(self, src, dst, device):
            n = count[0]
            count[0] += 1
            self.copy = pltpu.make_async_remote_copy(
                src_ref=src, dst_ref=dst, send_sem=ssem.at[n], recv_sem=rsem.at[n], device_id=device, device_id_type=MESH
            )

        def start(self):
            self.copy.start()
            sent.append(self.copy)
            return self

        def arrived(self):
            self.copy.wait_recv()

    local = []

    def load(src, dst):
        cp = pltpu.make_async_copy(src, dst, lsem.at[len(local)])
        local.append(cp)
        cp.start()
        return cp

    barrier = pltpu.get_barrier_semaphore()
    peers = [dev(0, 0, 1, 0), dev(0, 0, 2, 0), dev(0, 0, 3, 0), dev(0, 0, 0, 1)]
    peers += [dev(dz, dy, 0, 0) for dz, dy in (ZP, ZM, YP, YM, (2, 0), (0, 2))]
    for peer in peers:
        pl.semaphore_signal(barrier, inc=1, device_id=peer, device_id_type=MESH)

    here = y * 4 + z
    cp_mixed = load(mixed_h, ah.at[x])
    cp_slot = load(slot_h, meta.at[here])
    cp_wmix = load(wmix_h, wmix)
    cp_tok = load(tok_h, tok)
    cp_gain = load(gain_h, gain)
    cp_bg = load(bg_h, bg)
    cp_rw = load(rw_h, rw)

    cp_mixed.wait()
    cp_slot.wait()
    pl.semaphore_wait(barrier, len(peers))

    heads = {}
    for dx in (2, 1, 3):
        heads[(4 - dx) % 4] = Msg(ah.at[x], ah.at[x], dev(0, 0, dx, 0)).start()
    m_z = [Msg(meta.at[here], meta.at[here], dev(dz, 0, 0, 0)).start() for dz in (2, 1, 3)]

    cp_gate = load(gate_h, w.at[0:64])
    cp_up = load(up_h, w.at[128:192])
    w_p = [
        Msg(gate_h, w.at[64:128], dev(0, 0, 0, 1)).start(),
        Msg(up_h, w.at[192:256], dev(0, 0, 0, 1)).start(),
    ]
    cols = pl.ds(pl.multiple_of(x * 512, 512), 512)
    cp_down = load(down_h.at[:, cols], d.at[0:64])
    cp_ed = load(ed_h.at[:, cols], ed.at[0:256])
    cp_eg = load(eg_h, eg)
    cp_eu = load(eu_h, eu)
    down_x, ed_x = {}, {}
    for dx in (2, 1, 3):
        their = pl.ds(pl.multiple_of(lax.rem(x + dx, 4) * 512, 512), 512)
        s = (4 - dx) % 4
        down_x[s] = Msg(down_h.at[:, their], d.at[s * 128 : s * 128 + 64], dev(0, 0, dx, 0)).start()
        ed_x[s] = Msg(ed_h.at[:, their], ed.at[s * 256 : s * 256 + 256], dev(0, 0, dx, 0)).start()
    down_p = [Msg(down_h.at[:, cols], d.at[64:128], dev(0, 0, 0, 1)).start()]

    cp_wmix.wait()
    cp_tok.wait()
    cp_gain.wait()
    cp_bg.wait()

    def head_part(s, n):
        src = lax.rem(x + s, 4)
        rows = pl.ds(pl.multiple_of(src * 256, 256), 256)
        return dot(ah[src], wmix[rows, n * 512 : (n + 1) * 512])

    for n in range(4):
        s = slice(n * 512, (n + 1) * 512)
        macc[:, s] = tok[:, s].astype(F32) + head_part(0, n)
    for h in (1, 3):
        heads[h].arrived()
        for n in range(4):
            macc[:, n * 512 : (n + 1) * 512] += head_part(h, n)
    heads[2].arrived()
    sq = jnp.zeros((48, 1), F32)
    for n in range(4):
        s = slice(n * 512, (n + 1) * 512)
        r = (macc[:, s] + head_part(2, n)).astype(BF16)
        res[:, s] = r
        rf = r.astype(F32)
        sq = sq + jnp.sum(rf * rf, axis=-1, keepdims=True)
    inv = lax.rsqrt(sq * (1.0 / 2048.0) + EPS)
    for n in range(4):
        s = slice(n * 512, (n + 1) * 512)
        g[0, n] = (res[:, s].astype(F32) * inv * gain[:, s]).astype(BF16)

    def spread(rel, q0, nq, way):
        to = ((rel[0] - way[0]) % 4, (rel[1] - way[1]) % 4)
        q = pl.ds(q0, nq)
        return Msg(g.at[IDX[rel], q], g.at[IDX[to], q], dev(*way, 0, 0)).start()

    O = (0, 0)
    a_zp, a_zm = spread(O, 0, 2, ZP), spread(O, 0, 2, ZM)
    b_yp, b_ym = spread(O, 2, 2, YP), spread(O, 2, 2, YM)
    for m in m_z:
        m.arrived()
    col = pl.ds(y * 4, 4)
    m_y = [Msg(meta.at[col], meta.at[col], dev(0, dy, 0, 0)).start() for dy in (2, 1, 3)]
    a_yp, a_ym = spread(O, 0, 2, YP), spread(O, 0, 2, YM)
    b_zp, b_zm = spread(O, 2, 2, ZP), spread(O, 2, 2, ZM)

    gate_sum = jnp.zeros((48, 1), F32)
    for n in range(4):
        s = slice(n * 512, (n + 1) * 512)
        gate_sum = gate_sum + jnp.sum(g[0, n].astype(F32) * bg[:, s].astype(F32), axis=-1, keepdims=True)
    bw = jax.nn.sigmoid(gate_sum)
    cp_rw.wait()
    scol = as_columns(meta[here])
    rwc = as_columns(rw[...])

    a_zp.arrived()
    f_z0 = spread((3, 0), 0, 1, ZP)
    t_33, t_31 = spread((3, 0), 0, 2, YP), spread((3, 0), 0, 2, YM)
    a_zm.arrived()
    f_z1 = spread((1, 0), 1, 1, ZM)
    t_13, t_11 = spread((1, 0), 0, 2, YP), spread((1, 0), 0, 2, YM)
    b_yp.arrived()
    f_y2 = spread((0, 3), 2, 1, YP)
    u_33, u_13 = spread((0, 3), 2, 2, ZP), spread((0, 3), 2, 2, ZM)
    b_ym.arrived()
    f_y3 = spread((0, 1), 3, 1, YM)
    u_31, u_11 = spread((0, 1), 2, 2, ZP), spread((0, 1), 2, 2, ZM)
    a_yp.arrived()
    f_y0 = spread((0, 3), 0, 1, YP)
    a_ym.arrived()
    f_y1 = spread((0, 1), 1, 1, YM)
    b_zp.arrived()
    f_z2 = spread((3, 0), 2, 1, ZP)
    b_zm.arrived()
    f_z3 = spread((1, 0), 3, 1, ZM)

    def up_group(n):
        r0, nb = GROUPS[n]
        acc = None
        for q in range(4):
            part = dot_nt(g[r0 : r0 + nb, q].reshape(nb * 48, 512), w[:, q * 512 : (q + 1) * 512])
            acc = part if acc is None else acc + part
        ga, up = acc[:, 0:128], acc[:, 128:256]
        rows = pl.ds(r0 * 48, nb * 48)
        hid[rows, 0:128] = (ga * jax.nn.sigmoid(ga) * up).astype(BF16)
        out = {}
        for dx in (2, 1, 3):
            s = (4 - dx) % 4
            out[s] = Msg(hid.at[rows, 0:128], hid.at[rows, s * 128 : s * 128 + 128], dev(0, 0, dx, 0)).start()
        return out

    e_mine = (me * 16).astype(F32)
    e_other = ((zy * 2 + (1 - c)) * 16).astype(F32)

    def pick_group(n):
        r0, nb = GROUPS[n]
        lane8 = lax.broadcasted_iota(jnp.int32, (8, 48), 0).astype(F32)
        code = jnp.concatenate([lane8 + e_mine, lane8 + e_other], axis=0)
        for r in range(r0, r0 + nb):
            dz, dy = REL[r]
            m = meta[lax.rem(y + dy, 4) * 4 + lax.rem(z + dz, 4)]
            hit = jnp.where(m[0:1, 0:48] == code, 1.0, 0.0) + jnp.where(m[1:2, 0:48] == code, 1.0, 0.0)
            hit = hit.astype(BF16)
            for q in range(4):
                picked = dot(hit, g[r, q])
                s = slice(q * 512, (q + 1) * 512)
                xo[r * 8 : r * 8 + 8, s] = picked[0:8]
                xp[r * 8 : r * 8 + 8, s] = picked[8:16]

    def pass_rows(a, b):
        rows = slice(a, b)
        xs[rows] = xp[rows].astype(BF16)
        return Msg(xs.at[rows], xb.at[rows], dev(0, 0, 0, 1)).start()

    cp_gate.wait()
    cp_up.wait()
    for m in w_p:
        m.arrived()
    hid_in = {}
    hid_in[0] = up_group(0)
    for m in m_y:
        m.arrived()
    pick_group(0)

    f_z0.arrived()
    f_z1.arrived()
    t_23, t_21 = spread((2, 0), 0, 2, YP), spread((2, 0), 0, 2, YM)
    f_y2.arrived()
    f_y3.arrived()
    u_32, u_12 = spread((0, 2), 2, 2, ZP), spread((0, 2), 2, 2, ZM)
    t_33.arrived()
    h_32a = spread((3, 3), 0, 1, YP)
    t_31.arrived()
    h_32b = spread((3, 1), 1, 1, YM)
    t_13.arrived()
    h_12a = spread((1, 3), 0, 1, YP)
    t_11.arrived()
    h_12b = spread((1, 1), 1, 1, YM)
    u_33.arrived()
    h_23a = spread((3, 3), 2, 1, ZP)
    u_13.arrived()
    h_23b = spread((1, 3), 3, 1, ZM)
    u_31.arrived()
    h_21a = spread((3, 1), 2, 1, ZP)
    u_11.arrived()
    h_21b = spread((1, 1), 3, 1, ZM)
    for m in (f_y0, f_y1, f_z2, f_z3):
        m.arrived()

    hid_in[1] = up_group(1)

    t_23.arrived()
    l_22a = spread((2, 3), 0, 1, YP)
    t_21.arrived()
    l_22b = spread((2, 1), 1, 1, YM)
    u_32.arrived()
    l_22c = spread((3, 2), 2, 1, ZP)
    u_12.arrived()
    l_22d = spread((1, 2), 3, 1, ZM)

    cp_down.wait()
    for s in (1, 2, 3):
        down_x[s].arrived()
        own = slice(s * 128, s * 128 + 64)
        down_p.append(Msg(d.at[own], d.at[s * 128 + 64 : s * 128 + 128], dev(0, 0, 0, 1)).start())

    pick_group(1)

    for m in (h_32a, h_32b, h_12a, h_12b, h_23a, h_23b, h_21a, h_21b):
        m.arrived()
    hid_in[2] = up_group(2)
    pick_group(2)
    passed = pass_rows(0, 112)

    reduced = {}

    def down_group(n):
        r0, nb = GROUPS[n]
        for m in hid_in[n].values():
            m.arrived()
        part = dot(hid[r0 * 48 : (r0 + nb) * 48, :], d[...])
        for i in range(nb):
            r = r0 + i
            blk = part[i * 48 : (i + 1) * 48].astype(BF16)
            if r == 0:
                rsr[0] = blk
            else:
                dz, dy = REL[r]
                sb[r] = blk
                back = IDX[((-dz) % 4, (-dy) % 4)]
                reduced[back] = Msg(sb.at[r], rsr.at[back], dev(dz, dy, 0, 0)).start()

    for m in down_p:
        m.arrived()
    down_group(0)

    cp_eg.wait()
    cp_eu.wait()

    def expert_up(rows_in):
        ga = dot(rows_in, eg[...])
        up = dot(rows_in, eu[...])
        return (ga * jax.nn.sigmoid(ga) * up).astype(BF16)

    def send_hidden(ref):
        out = []
        for dx in (2, 1, 3):
            s = (4 - dx) % 4
            out.append(Msg(ref.at[:, 0:256], ref.at[:, s * 256 : s * 256 + 256], dev(0, 0, dx, 0)).start())
        return out

    eh[0, :, 0:256] = expert_up(xo[0:112].astype(BF16))
    eh_in = send_hidden(eh.at[0])
    down_group(1)
    passed.arrived()
    eh[1, :, 0:256] = expert_up(xb[0:112])
    eh_in += send_hidden(eh.at[1])

    for m in (l_22a, l_22b, l_22c, l_22d):
        m.arrived()
    pick_group(3)
    passed = pass_rows(112, 128)
    hid_in[3] = up_group(3)
    down_group(2)
    passed.arrived()
    el[:, 0:256] = expert_up(jnp.concatenate([xo[112:128].astype(BF16), xb[112:128]], axis=0))
    el_in = send_hidden(el)

    cp_ed.wait()
    for m in ed_x.values():
        m.arrived()
    returned = []

    def give_back(half, r, eo):
        blk = jnp.concatenate([eo[:, 0:256], eo[:, 256:512]], axis=0).astype(BF16)
        if r == 0 and half == 0:
            eret[me] = blk
        else:
            dz, dy = REL[r]
            rb[half, r] = blk
            returned.append(Msg(rb.at[half, r], eret.at[me], dev(dz, dy, 0, half)).start())

    for m in eh_in:
        m.arrived()
    eo = dot(eh[...].reshape(224, 1024), ed[...])
    for r in range(13, -1, -1):
        for half in range(2):
            give_back(half, r, eo[half * 112 + r * 8 : half * 112 + r * 8 + 8])
    down_group(3)
    for m in el_in:
        m.arrived()
    eo = dot(el[...], ed[...])
    for r in (15, 14):
        for half in range(2):
            give_back(half, r, eo[half * 16 + (r - 14) * 8 : half * 16 + (r - 14) * 8 + 8])

    lane = lax.broadcasted_iota(jnp.int32, (48, 512), 1).astype(F32)
    sel = jnp.concatenate(
        [jnp.where(lane == scol[0:48, ch : ch + 1] + float(hf * 8), 1.0, 0.0) for hf in range(2) for ch in range(2)], axis=0
    ).astype(BF16)
    total = rsr[0].astype(F32)
    for r in range(1, 16):
        reduced[r].arrived()
        total = total + rsr[r].astype(F32)
    base = res[:, cols].astype(F32) + bw * total
    for m in returned:
        m.arrived()
    got = dot(sel, eret[...].reshape(512, 256))
    for hf in range(2):
        s = slice(hf * 256, hf * 256 + 256)
        first, second = got[hf * 96 : hf * 96 + 48], got[hf * 96 + 48 : hf * 96 + 96]
        out[:, s] = (base[:, s] + first * rwc[0:48, 0:1] + second * rwc[0:48, 1:2]).astype(BF16)

    for cp in sent:
        cp.wait_send()


def layer_call(*args):
    any_ = pl.BlockSpec(memory_space=pl.ANY)
    vm = pl.BlockSpec(memory_space=pltpu.VMEM)
    return pl.pallas_call(
        layer_kernel,
        out_shape=jax.ShapeDtypeStruct((48, 512), BF16),
        in_specs=[any_] * 13,
        out_specs=vm,
        scratch_shapes=[
            pltpu.VMEM((4, 48, 256), BF16),
            pltpu.VMEM((48, 2048), BF16),
            pltpu.VMEM((1024, 2048), BF16),
            pltpu.VMEM((1, 2048), F32),
            pltpu.VMEM((1, 2048), BF16),
            pltpu.VMEM((48, 2048), F32),
            pltpu.VMEM((2, 48), F32),
            pltpu.VMEM((256, 2048), BF16),
            pltpu.VMEM((512, 512), BF16),
            pltpu.VMEM((2048, 256), BF16),
            pltpu.VMEM((2048, 256), BF16),
            pltpu.VMEM((1024, 512), BF16),
            pltpu.VMEM((16, 8, 128), F32),
            pltpu.VMEM((16, 4, 48, 512), BF16),
            pltpu.VMEM((48, 2048), BF16),
            pltpu.VMEM((768, 512), BF16),
            pltpu.VMEM((128, 2048), F32),
            pltpu.VMEM((128, 2048), F32),
            pltpu.VMEM((128, 2048), BF16),
            pltpu.VMEM((128, 2048), BF16),
            pltpu.VMEM((2, 112, 1024), BF16),
            pltpu.VMEM((32, 1024), BF16),
            pltpu.VMEM((16, 48, 512), BF16),
            pltpu.VMEM((16, 48, 512), BF16),
            pltpu.VMEM((2, 16, 16, 256), BF16),
            pltpu.VMEM((32, 16, 256), BF16),
            pltpu.SemaphoreType.DMA((N_MSG,)),
            pltpu.SemaphoreType.DMA((N_MSG,)),
            pltpu.SemaphoreType.DMA((16,)),
        ],
        compiler_params=pltpu.CompilerParams(vmem_limit_bytes=67043328, collective_id=0, has_side_effects=True),
        name="layer",
    )(*args)


def local(
    tokens, mix_gain, w_query, w_key, w_value, w_outgate, w_ingate, w_forget, in_bias, forget_bias, w_mix_out,
    cell_state, norm_state, max_state, moe_gain, route_ids, route_weights, expert_gate, expert_up, expert_down,
    branch_gate, dense_gate, dense_up, dense_down,
):
    mixed, new_cell, new_norm, new_max, slots = cell_call(
        tokens, mix_gain.reshape(1, 2048), w_query, w_key, w_value, w_outgate, w_ingate.T, w_forget.T,
        in_bias, forget_bias, cell_state, norm_state.reshape(96, 128), max_state.T, route_ids.T,
    )
    layer_out = layer_call(
        mixed, tokens, w_mix_out, moe_gain.reshape(1, 2048), branch_gate.reshape(1, 2048), slots, route_weights.T,
        dense_gate.T, dense_up.T, dense_down,
        expert_gate.reshape(2048, 256), expert_up.reshape(2048, 256), expert_down.reshape(256, 2048),
    )
    return (layer_out, new_cell, new_norm.reshape(48, 2, 128), new_max.T)


def solution(mesh):
    in_specs = (
        P("ep", None),
        P(),
        P(None, "tp"),
        P(None, "tp"),
        P(None, "tp"),
        P(None, "tp"),
        P(None, "tp"),
        P(None, "tp"),
        P("tp"),
        P("tp"),
        P(),
        P("ep", "tp", None, None),
        P("ep", "tp", None),
        P("ep", "tp"),
        P(),
        P("ep", None),
        P("ep", None),
        P("ep", None, "tp"),
        P("ep", None, "tp"),
        P("ep", "tp", None),
        P(),
        P(None, ("ep", "tp")),
        P(None, ("ep", "tp")),
        P(("ep", "tp"), None),
    )
    out_specs = (P("ep", "tp"), P("ep", "tp", None, None), P("ep", "tp", None), P("ep", "tp"))
    return jax.shard_map(local, mesh=mesh, in_specs=in_specs, out_specs=out_specs, check_vma=False)
```

```python
import functools

import jax
import jax.numpy as jnp
from jax import lax
from jax.experimental import pallas as pl
from jax.experimental.pallas import tpu as pltpu
from jax.sharding import PartitionSpec as P

EPS = 1e-06
MESH = pl.DeviceIdType.MESH
F32 = jnp.float32
BF16 = jnp.bfloat16
NT = (((1,), (1,)), ((), ()))


def dot(a, b):
    return jnp.dot(a, b, preferred_element_type=F32)


def dot_nt(a, b):
    return lax.dot_general(a, b, NT, preferred_element_type=F32)


CHUNK = 6
N_CHUNK = 8


def split3(a):
    first = a.astype(BF16).astype(F32)
    rest = a - first
    second = rest.astype(BF16).astype(F32)
    return first, second, rest - second


def as_columns(rows):
    n, width = rows.shape
    wide = jnp.concatenate([rows, jnp.zeros((n, 128 - width), F32)], axis=1) if width < 128 else rows
    return jnp.concatenate([wide, jnp.zeros((128 - n, 128), F32)], axis=0).T


def slot_rows(ids):
    idf = ids.astype(F32)
    idc = as_columns(idf)
    before = lax.broadcasted_iota(jnp.int32, (48, 48), 0) < lax.broadcasted_iota(jnp.int32, (48, 48), 1)
    slots = []
    for ch in range(2):
        row = idf[ch : ch + 1, :]
        hits = jnp.where(idc[0:48, 0:1] == row, 1.0, 0.0) + jnp.where(idc[0:48, 1:2] == row, 1.0, 0.0)
        rank = jnp.sum(jnp.where(before, hits, 0.0), axis=0, keepdims=True)
        slots.append(row * 16.0 + rank)
    srow = jnp.concatenate(slots + [jnp.zeros((6, 48), F32)], axis=0)
    return jnp.concatenate([srow, jnp.zeros((8, 80), F32)], axis=1)


REL = [
    (0, 0), (1, 0), (3, 0), (0, 1), (0, 3),
    (1, 1), (1, 3), (3, 1), (3, 3), (2, 0), (0, 2),
    (2, 1), (2, 3), (1, 2), (3, 2),
    (2, 2),
]
IDX = {rel: i for i, rel in enumerate(REL)}
GROUPS = [(0, 5), (5, 6), (11, 4), (15, 1)]
ZP, ZM, YP, YM = (1, 0), (3, 0), (0, 1), (0, 3)
N_MSG = 160


def layer_kernel(
    tok_h, cgain_h, wq_h, wk_h, wv_h, wo_h, win_h, wf_h, inb_h, fb_h, cell_h, norm_h, max_h, ids_h,
    wmix_h, gain_h, bg_h, rw_h, gate_h, up_h, down_h, eg_h, eu_h, ed_h,
    out, cell, norm_o, max_o,
    inb, fb, tok, cgain, wts, win, wf, norm, mx, ids, normed, vs, vf, cb, qt, wt, num, wsem, csem, msem,
    ah, wmix, gain, bg, macc, rw, w, d, eg, eu, ed, meta, g, res, hid, xo, xp, xb, xs, eh, el, sb, rsr, rb, eret,
    ssem, rsem, lsem,
):
    me = lax.axis_index("ep")
    x = lax.axis_index("tp")
    c = lax.rem(me, 2)
    zy = lax.div(me, 2)
    y = lax.rem(zy, 4)
    z = lax.div(zy, 4)

    def dev(dz, dy, dx, pc):
        zz = lax.rem(z + dz, 4)
        yy = lax.rem(y + dy, 4)
        cc = 1 - c if pc else c
        return ((zz * 4 + yy) * 2 + cc, lax.rem(x + dx, 4))

    count = [0]
    sent = []

    class Msg:
        def __init__(self, src, dst, device):
            n = count[0]
            count[0] += 1
            self.copy = pltpu.make_async_remote_copy(
                src_ref=src, dst_ref=dst, send_sem=ssem.at[n], recv_sem=rsem.at[n], device_id=device, device_id_type=MESH
            )

        def start(self):
            self.copy.start()
            sent.append(self.copy)
            return self

        def arrived(self):
            self.copy.wait_recv()

    local = []

    def load(src, dst):
        cp = pltpu.make_async_copy(src, dst, lsem.at[len(local)])
        local.append(cp)
        cp.start()
        return cp

    barrier = pltpu.get_barrier_semaphore()
    peers = [dev(0, 0, 1, 0), dev(0, 0, 2, 0), dev(0, 0, 3, 0), dev(0, 0, 0, 1)]
    peers += [dev(dz, dy, 0, 0) for dz, dy in (ZP, ZM, YP, YM, (2, 0), (0, 2))]
    for peer in peers:
        pl.semaphore_signal(barrier, inc=1, device_id=peer, device_id_type=MESH)

    here = y * 4 + z
    cols = pl.ds(pl.multiple_of(x * 512, 512), 512)

    small = [
        pltpu.make_async_copy(src, dst, msem.at[i])
        for i, (src, dst) in enumerate(
            [(tok_h, tok), (cgain_h, cgain), (win_h, win), (wf_h, wf), (max_h, mx), (norm_h, norm), (ids_h, ids), (inb_h, inb), (fb_h, fb)]
        )
    ]
    for cp in small[0:2]:
        cp.start()
    wcp = [pltpu.make_async_copy(src, wts.at[i], wsem.at[i]) for i, src in enumerate([wq_h, wk_h, wv_h, wo_h])]
    wcp[0].start()
    for cp in small[2:]:
        cp.start()
    for cp in wcp[1:]:
        cp.start()

    def cin(i):
        s = pl.ds(i * CHUNK, CHUNK)
        return pltpu.make_async_copy(cell_h.at[s], cell.at[s], csem.at[i])

    for cp in small[0:2]:
        cp.wait()
    for i in range(N_CHUNK):
        cin(i).start()
    xf = tok[...].astype(F32)
    ms = jnp.mean(xf * xf, axis=-1, keepdims=True)
    normed[...] = (xf * lax.rsqrt(ms + EPS) * cgain[...]).astype(BF16)
    nb = normed[...]
    for cp in small[2:]:
        cp.wait()
    meta[here] = slot_rows(ids[...])
    in_pre = dot_nt(win[...], nb)
    fpre = dot_nt(wf[...], nb)
    hrow = lax.broadcasted_iota(jnp.int32, in_pre.shape, 0)
    in_pre = in_pre + jnp.where(hrow == 0, inb[0], inb[1])
    fpre = fpre + jnp.where(hrow == 0, fb[0], fb[1])
    log_f = jnp.minimum(fpre, 0.0) - jnp.log1p(jnp.exp(-jnp.abs(fpre)))
    lm = log_f + mx[...]
    new_max = jnp.maximum(lm, in_pre)
    max_o[...] = new_max
    carry = jnp.exp(lm - new_max)
    write = jnp.exp(in_pre - new_max)
    floor = jnp.exp(-new_max)
    rows = jnp.concatenate([carry, write, floor], axis=0)
    rows = jnp.concatenate([rows, jnp.zeros((6, 80), F32)], axis=1)
    rows = jnp.concatenate([rows, jnp.zeros((122, 128), F32)], axis=0)
    gcols = rows.T

    wcp[0].wait()
    q = dot(nb, wts[0])
    wcp[1].wait()
    k = dot(nb, wts[1]) * (128 ** (-0.5))
    wcp[2].wait()
    v = dot(nb, wts[2])
    for h in range(2):
        v1, v2, _ = split3(v[:, h * 128 : (h + 1) * 128])
        vs[h] = jnp.concatenate([v1, v1, v2], axis=0).astype(BF16)
        vf[h] = v[:, h * 128 : (h + 1) * 128]
    cp_wmix = load(wmix_h, wmix)
    cp_gain = load(gain_h, gain)
    cp_bg = load(bg_h, bg)
    cp_rw = load(rw_h, rw)
    cp_gate = load(gate_h, w.at[0:64])
    cp_up = load(up_h, w.at[128:192])
    cp_down = load(down_h.at[:, cols], d.at[0:64])
    cp_ed = load(ed_h.at[:, cols], ed.at[0:256])
    cp_eg = load(eg_h, eg)
    cp_eu = load(eu_h, eu)
    wcp[3].wait()
    og = jax.nn.sigmoid(dot(nb, wts[3]))

    pl.semaphore_wait(barrier, len(peers))
    w_p = [
        Msg(gate_h, w.at[64:128], dev(0, 0, 0, 1)).start(),
        Msg(up_h, w.at[192:256], dev(0, 0, 0, 1)).start(),
    ]
    down_p = [Msg(down_h.at[:, cols], d.at[64:128], dev(0, 0, 0, 1)).start()]
    down_x, ed_x = {}, {}

    def their(dx):
        return pl.ds(pl.multiple_of(lax.rem(x + dx, 4) * 512, 512), 512)

    def send_ed(dx):
        s = (4 - dx) % 4
        ed_x[s] = Msg(ed_h.at[:, their(dx)], ed.at[s * 256 : s * 256 + 256], dev(0, 0, dx, 0)).start()

    for dx in (2, 1, 3):
        s = (4 - dx) % 4
        down_x[s] = Msg(down_h.at[:, their(dx)], d.at[s * 128 : s * 128 + 64], dev(0, 0, dx, 0)).start()

    m_z = [Msg(meta.at[here], meta.at[here], dev(dz, 0, 0, 0)).start() for dz in (2, 1, 3)]

    denom = []
    pad = jnp.zeros((112, 128), F32)
    for h in range(2):
        ca = jnp.broadcast_to(gcols[0:48, h : h + 1], (48, 128))
        wr = jnp.broadcast_to(gcols[0:48, 2 + h : 3 + h], (48, 128))
        qh = q[:, h * 128 : (h + 1) * 128]
        written = wr * k[:, h * 128 : (h + 1) * 128]
        hs = pl.ds(h, 48, stride=2)
        nn = ca * norm[hs, :] + written
        norm_o[hs, :] = nn
        den = jnp.sum(qh * nn, axis=-1, keepdims=True)
        denom.append(jnp.maximum(jnp.abs(den), gcols[0:48, 4 + h : 5 + h]))
        cb[h] = ca
        vf[h] = jnp.sum(qh * written, axis=-1, keepdims=True) * vf[h]
        q1, q2, q3 = split3(qh)
        qt[h] = jnp.concatenate([q1, q2, q3, pad], axis=0).T[:, 0:144].astype(BF16)
        w1, w2, _ = split3(written)
        wt[h] = jnp.concatenate([w1, w2, w1, pad], axis=0).T[:, 0:144].astype(BF16)

    token = lax.rem(lax.broadcasted_iota(jnp.int32, (144, 128), 0), 48)

    def tokens_of(i):
        return [token == i * CHUNK + j for j in range(CHUNK)]

    def read_step(i, _):
        cin(i).wait()
        ones = jnp.concatenate([jnp.where(m, 1.0, 0.0) for m in tokens_of(i)], axis=1).astype(BF16)
        for h in range(2):
            qcols = dot(qt[h], ones)
            for j in range(CHUNK):
                b = i * CHUNK + j
                num[h, pl.ds(b, 1), :] = jnp.sum(
                    qcols[:, j * 128 : (j + 1) * 128] * cell[b, h], axis=0, keepdims=True
                )
        return 0

    def write_step(i, _):
        here = tokens_of(i)
        for h in range(2):
            vh = vs[h].astype(F32)
            vrows = jnp.concatenate([jnp.where(m, vh, 0.0) for m in here], axis=1).astype(BF16)
            outer = dot(wt[h], vrows)
            for j in range(CHUNK):
                b = i * CHUNK + j
                cell[b, h] = cb[h, pl.ds(b, 1), :] * cell[b, h] + outer[:, j * 128 : (j + 1) * 128]
        return 0

    lax.fori_loop(0, N_CHUNK, read_step, 0)
    for h in range(2):
        lanes = slice(h * 128, (h + 1) * 128)
        ah[x, :, lanes] = (og[:, lanes] * ((cb[h] * num[h] + vf[h]) / denom[h])).astype(BF16)

    heads = {}
    for dx in (2, 1, 3):
        heads[(4 - dx) % 4] = Msg(ah.at[x], ah.at[x], dev(0, 0, dx, 0)).start()

    cp_wmix.wait()
    cp_gain.wait()
    cp_bg.wait()

    def head_part(s, n):
        src = lax.rem(x + s, 4)
        rows = pl.ds(pl.multiple_of(src * 256, 256), 256)
        return dot(ah[src], wmix[rows, n * 512 : (n + 1) * 512])

    for n in range(4):
        s = slice(n * 512, (n + 1) * 512)
        macc[:, s] = tok[:, s].astype(F32) + head_part(0, n)
    for h in (1, 3):
        heads[h].arrived()
        for n in range(4):
            macc[:, n * 512 : (n + 1) * 512] += head_part(h, n)
    heads[2].arrived()
    sq = jnp.zeros((48, 1), F32)
    for n in range(4):
        s = slice(n * 512, (n + 1) * 512)
        r = (macc[:, s] + head_part(2, n)).astype(BF16)
        res[:, s] = r
        rf = r.astype(F32)
        sq = sq + jnp.sum(rf * rf, axis=-1, keepdims=True)
    inv = lax.rsqrt(sq * (1.0 / 2048.0) + EPS)
    for n in range(4):
        s = slice(n * 512, (n + 1) * 512)
        g[0, n] = (res[:, s].astype(F32) * inv * gain[:, s]).astype(BF16)

    def spread(rel, q0, nq, way):
        to = ((rel[0] - way[0]) % 4, (rel[1] - way[1]) % 4)
        q = pl.ds(q0, nq)
        return Msg(g.at[IDX[rel], q], g.at[IDX[to], q], dev(*way, 0, 0)).start()

    O = (0, 0)
    a_zp, a_zm = spread(O, 0, 2, ZP), spread(O, 0, 2, ZM)
    b_yp, b_ym = spread(O, 2, 2, YP), spread(O, 2, 2, YM)
    for m in m_z:
        m.arrived()
    col = pl.ds(y * 4, 4)
    m_y = [Msg(meta.at[col], meta.at[col], dev(0, dy, 0, 0)).start() for dy in (2, 1, 3)]
    a_yp, a_ym = spread(O, 0, 2, YP), spread(O, 0, 2, YM)
    b_zp, b_zm = spread(O, 2, 2, ZP), spread(O, 2, 2, ZM)

    for dx in (2, 1, 3):
        send_ed(dx)

    lax.fori_loop(0, N_CHUNK, write_step, 0)

    gate_sum = jnp.zeros((48, 1), F32)
    gate_rows = bg[...].astype(F32)
    for n in range(4):
        rowsum = jnp.zeros((48, 128), F32)
        for i in range(4):
            rowsum = rowsum + g[0, n, :, i * 128 : (i + 1) * 128].astype(F32) * gate_rows[n * 4 + i : n * 4 + i + 1]
        gate_sum = gate_sum + jnp.sum(rowsum, axis=-1, keepdims=True)
    bw = jax.nn.sigmoid(gate_sum)
    cp_rw.wait()
    scol = as_columns(meta[here])
    rwc = as_columns(rw[...])

    a_zp.arrived()
    f_z0 = spread((3, 0), 0, 1, ZP)
    t_33, t_31 = spread((3, 0), 0, 2, YP), spread((3, 0), 0, 2, YM)
    a_zm.arrived()
    f_z1 = spread((1, 0), 1, 1, ZM)
    t_13, t_11 = spread((1, 0), 0, 2, YP), spread((1, 0), 0, 2, YM)
    b_yp.arrived()
    f_y2 = spread((0, 3), 2, 1, YP)
    u_33, u_13 = spread((0, 3), 2, 2, ZP), spread((0, 3), 2, 2, ZM)
    b_ym.arrived()
    f_y3 = spread((0, 1), 3, 1, YM)
    u_31, u_11 = spread((0, 1), 2, 2, ZP), spread((0, 1), 2, 2, ZM)
    a_yp.arrived()
    f_y0 = spread((0, 3), 0, 1, YP)
    a_ym.arrived()
    f_y1 = spread((0, 1), 1, 1, YM)
    b_zp.arrived()
    f_z2 = spread((3, 0), 2, 1, ZP)
    b_zm.arrived()
    f_z3 = spread((1, 0), 3, 1, ZM)

    def up_group(n):
        r0, nb = GROUPS[n]
        acc = None
        for q in range(4):
            part = dot_nt(g[r0 : r0 + nb, q].reshape(nb * 48, 512), w[:, q * 512 : (q + 1) * 512])
            acc = part if acc is None else acc + part
        ga, up = acc[:, 0:128], acc[:, 128:256]
        rows = pl.ds(r0 * 48, nb * 48)
        hid[rows, 0:128] = (ga * jax.nn.sigmoid(ga) * up).astype(BF16)
        out = {}
        for dx in (2, 1, 3):
            s = (4 - dx) % 4
            out[s] = Msg(hid.at[rows, 0:128], hid.at[rows, s * 128 : s * 128 + 128], dev(0, 0, dx, 0)).start()
        return out

    e_mine = (me * 16).astype(F32)
    e_other = ((zy * 2 + (1 - c)) * 16).astype(F32)

    def pick_group(n):
        r0, nb = GROUPS[n]
        lane8 = lax.broadcasted_iota(jnp.int32, (8, 48), 0).astype(F32)
        code = jnp.concatenate([lane8 + e_mine, lane8 + e_other], axis=0)
        for r in range(r0, r0 + nb):
            dz, dy = REL[r]
            m = meta[lax.rem(y + dy, 4) * 4 + lax.rem(z + dz, 4)]
            hit = jnp.where(m[0:1, 0:48] == code, 1.0, 0.0) + jnp.where(m[1:2, 0:48] == code, 1.0, 0.0)
            hit = hit.astype(BF16)
            for q in range(4):
                picked = dot(hit, g[r, q])
                s = slice(q * 512, (q + 1) * 512)
                xo[r * 8 : r * 8 + 8, s] = picked[0:8]
                xp[r * 8 : r * 8 + 8, s] = picked[8:16]

    def pass_rows(a, b):
        rows = slice(a, b)
        xs[rows] = xp[rows].astype(BF16)
        return Msg(xs.at[rows], xb.at[rows], dev(0, 0, 0, 1)).start()

    cp_down.wait()
    for s in (1, 2, 3):
        down_x[s].arrived()
        own = slice(s * 128, s * 128 + 64)
        down_p.append(Msg(d.at[own], d.at[s * 128 + 64 : s * 128 + 128], dev(0, 0, 0, 1)).start())

    cp_gate.wait()
    cp_up.wait()
    for m in w_p:
        m.arrived()
    hid_in = {}
    hid_in[0] = up_group(0)
    for m in m_y:
        m.arrived()
    pick_group(0)

    f_z0.arrived()
    f_z1.arrived()
    t_23, t_21 = spread((2, 0), 0, 2, YP), spread((2, 0), 0, 2, YM)
    f_y2.arrived()
    f_y3.arrived()
    u_32, u_12 = spread((0, 2), 2, 2, ZP), spread((0, 2), 2, 2, ZM)
    t_33.arrived()
    h_32a = spread((3, 3), 0, 1, YP)
    t_31.arrived()
    h_32b = spread((3, 1), 1, 1, YM)
    t_13.arrived()
    h_12a = spread((1, 3), 0, 1, YP)
    t_11.arrived()
    h_12b = spread((1, 1), 1, 1, YM)
    u_33.arrived()
    h_23a = spread((3, 3), 2, 1, ZP)
    u_13.arrived()
    h_23b = spread((1, 3), 3, 1, ZM)
    u_31.arrived()
    h_21a = spread((3, 1), 2, 1, ZP)
    u_11.arrived()
    h_21b = spread((1, 1), 3, 1, ZM)
    for m in (f_y0, f_y1, f_z2, f_z3):
        m.arrived()

    hid_in[1] = up_group(1)

    t_23.arrived()
    l_22a = spread((2, 3), 0, 1, YP)
    t_21.arrived()
    l_22b = spread((2, 1), 1, 1, YM)
    u_32.arrived()
    l_22c = spread((3, 2), 2, 1, ZP)
    u_12.arrived()
    l_22d = spread((1, 2), 3, 1, ZM)

    reduced = {}

    def down_group(n):
        r0, nb = GROUPS[n]
        for m in hid_in[n].values():
            m.arrived()
        part = dot(hid[r0 * 48 : (r0 + nb) * 48, :], d[...])
        for i in range(nb):
            r = r0 + i
            blk = part[i * 48 : (i + 1) * 48].astype(BF16)
            if r == 0:
                rsr[0] = blk
            else:
                dz, dy = REL[r]
                sb[r] = blk
                back = IDX[((-dz) % 4, (-dy) % 4)]
                reduced[back] = Msg(sb.at[r], rsr.at[back], dev(dz, dy, 0, 0)).start()

    pick_group(1)
    first_rows = pass_rows(0, 80)
    for m in down_p:
        m.arrived()
    down_group(0)
    for m in (h_32a, h_32b, h_12a, h_12b, h_23a, h_23b, h_21a, h_21b):
        m.arrived()
    hid_in[2] = up_group(2)
    pick_group(2)
    passed = [pass_rows(80, 112)]
    down_group(1)

    cp_eg.wait()
    cp_eu.wait()

    def expert_up(ref, a, b):
        rows_in = jnp.concatenate([xo[a:b].astype(BF16), xb[a:b]], axis=0)
        ga = dot(rows_in, eg[...])
        up = dot(rows_in, eu[...])
        ref[:, 0:256] = (ga * jax.nn.sigmoid(ga) * up).astype(BF16)
        out = []
        for dx in (2, 1, 3):
            s = (4 - dx) % 4
            out.append(Msg(ref.at[:, 0:256], ref.at[:, s * 256 : s * 256 + 256], dev(0, 0, dx, 0)).start())
        return out

    first_rows.arrived()
    eh_in = expert_up(eh, 0, 80)

    for m in (l_22a, l_22b, l_22c, l_22d):
        m.arrived()
    pick_group(3)
    passed.append(pass_rows(112, 128))
    hid_in[3] = up_group(3)
    for m in passed:
        m.arrived()
    el_in = expert_up(el, 80, 128)
    down_group(2)
    down_group(3)

    cp_ed.wait()
    for m in ed_x.values():
        m.arrived()
    returned = []

    def give_back(half, r, eo):
        blk = jnp.concatenate([eo[:, 0:256], eo[:, 256:512]], axis=0).astype(BF16)
        if r == 0 and half == 0:
            eret[me] = blk
        else:
            dz, dy = REL[r]
            rb[half, r] = blk
            returned.append(Msg(rb.at[half, r], eret.at[me], dev(dz, dy, 0, half)).start())

    for m in eh_in:
        m.arrived()
    eo = dot(eh[...], ed[...])
    for r in range(9, -1, -1):
        for half in range(2):
            give_back(half, r, eo[half * 80 + r * 8 : half * 80 + r * 8 + 8])
    for m in el_in:
        m.arrived()
    eo = dot(el[...], ed[...])
    for r in range(15, 9, -1):
        for half in range(2):
            give_back(half, r, eo[half * 48 + (r - 10) * 8 : half * 48 + (r - 10) * 8 + 8])

    lane = lax.broadcasted_iota(jnp.int32, (48, 512), 1).astype(F32)
    sel = jnp.concatenate(
        [jnp.where(lane == scol[0:48, ch : ch + 1] + float(hf * 8), 1.0, 0.0) for hf in range(2) for ch in range(2)], axis=0
    ).astype(BF16)
    total = rsr[0].astype(F32)
    for r in range(1, 16):
        reduced[r].arrived()
        total = total + rsr[r].astype(F32)
    base = res[:, cols].astype(F32) + bw * total
    for m in returned:
        m.arrived()
    got = dot(sel, eret[...].reshape(512, 256))
    for hf in range(2):
        s = slice(hf * 256, hf * 256 + 256)
        first, second = got[hf * 96 : hf * 96 + 48], got[hf * 96 + 48 : hf * 96 + 96]
        out[:, s] = (base[:, s] + first * rwc[0:48, 0:1] + second * rwc[0:48, 1:2]).astype(BF16)

    for cp in sent:
        cp.wait_send()


def layer_call(*args):
    vm = pl.BlockSpec(memory_space=pltpu.VMEM)
    args = [pltpu.with_memory_space_constraint(a, pltpu.HBM) for a in args]
    return pl.pallas_call(
        layer_kernel,
        out_shape=(
            jax.ShapeDtypeStruct((48, 512), BF16),
            jax.ShapeDtypeStruct((48, 2, 128, 128), F32),
            jax.ShapeDtypeStruct((96, 128), F32),
            jax.ShapeDtypeStruct((2, 48), F32),
        ),
        in_specs=[pl.BlockSpec(memory_space=pltpu.HBM)] * 24,
        out_specs=(vm, vm, vm, vm),
        scratch_shapes=[
            pltpu.SMEM((2,), F32),
            pltpu.SMEM((2,), F32),
            pltpu.VMEM((48, 2048), BF16),
            pltpu.VMEM((1, 2048), F32),
            pltpu.VMEM((4, 2048, 256), BF16),
            pltpu.VMEM((2, 2048), BF16),
            pltpu.VMEM((2, 2048), BF16),
            pltpu.VMEM((96, 128), F32),
            pltpu.VMEM((2, 48), F32),
            pltpu.VMEM((2, 48), jnp.int32),
            pltpu.VMEM((48, 2048), BF16),
            pltpu.VMEM((2, 144, 128), BF16),
            pltpu.VMEM((2, 48, 128), F32),
            pltpu.VMEM((2, 48, 128), F32),
            pltpu.VMEM((2, 128, 144), BF16),
            pltpu.VMEM((2, 128, 144), BF16),
            pltpu.VMEM((2, 48, 128), F32),
            pltpu.SemaphoreType.DMA((4,)),
            pltpu.SemaphoreType.DMA((N_CHUNK,)),
            pltpu.SemaphoreType.DMA((9,)),
            pltpu.VMEM((4, 48, 256), BF16),
            pltpu.VMEM((1024, 2048), BF16),
            pltpu.VMEM((1, 2048), F32),
            pltpu.VMEM((16, 128), BF16),
            pltpu.VMEM((48, 2048), F32),
            pltpu.VMEM((2, 48), F32),
            pltpu.VMEM((256, 2048), BF16),
            pltpu.VMEM((512, 512), BF16),
            pltpu.VMEM((2048, 256), BF16),
            pltpu.VMEM((2048, 256), BF16),
            pltpu.VMEM((1024, 512), BF16),
            pltpu.VMEM((16, 8, 128), F32),
            pltpu.VMEM((16, 4, 48, 512), BF16),
            pltpu.VMEM((48, 2048), BF16),
            pltpu.VMEM((768, 512), BF16),
            pltpu.VMEM((128, 2048), F32),
            pltpu.VMEM((128, 2048), F32),
            pltpu.VMEM((128, 2048), BF16),
            pltpu.VMEM((128, 2048), BF16),
            pltpu.VMEM((160, 1024), BF16),
            pltpu.VMEM((96, 1024), BF16),
            pltpu.VMEM((16, 48, 512), BF16),
            pltpu.VMEM((16, 48, 512), BF16),
            pltpu.VMEM((2, 16, 16, 256), BF16),
            pltpu.VMEM((32, 16, 256), BF16),
            pltpu.SemaphoreType.DMA((N_MSG,)),
            pltpu.SemaphoreType.DMA((N_MSG,)),
            pltpu.SemaphoreType.DMA((16,)),
        ],
        compiler_params=pltpu.CompilerParams(vmem_limit_bytes=44 * 2**20, collective_id=0, has_side_effects=True),
        name="layer",
    )(*args)


def finish_kernel(lay, cell, norm, mx, lay_o, cell_o, norm_o, max_o, sem):
    copies = [
        pltpu.make_async_copy(cell.at[12 * i : 12 * i + 12], cell_o.at[12 * i : 12 * i + 12], sem.at[i]) for i in range(4)
    ]
    copies.append(pltpu.make_async_copy(lay, lay_o, sem.at[4]))
    copies.append(pltpu.make_async_copy(norm, norm_o, sem.at[5]))
    copies.append(pltpu.make_async_copy(mx, max_o, sem.at[6]))
    for cp in copies:
        cp.start()
    for cp in copies:
        cp.wait()


def finish_call(*args):
    any_ = pl.BlockSpec(memory_space=pl.ANY)
    vm = pl.BlockSpec(memory_space=pltpu.VMEM)
    return pl.pallas_call(
        finish_kernel,
        out_shape=tuple(jax.ShapeDtypeStruct(a.shape, a.dtype) for a in args),
        in_specs=[vm] * 4,
        out_specs=[any_] * 4,
        scratch_shapes=[pltpu.SemaphoreType.DMA((7,))],
        compiler_params=pltpu.CompilerParams(vmem_limit_bytes=16 * 2**20),
        name="finish",
    )(*[pltpu.with_memory_space_constraint(a, pltpu.VMEM) for a in args])


def local(
    tokens, mix_gain, w_query, w_key, w_value, w_outgate, w_ingate, w_forget, in_bias, forget_bias, w_mix_out,
    cell_state, norm_state, max_state, moe_gain, route_ids, route_weights, expert_gate, expert_up, expert_down,
    branch_gate, dense_gate, dense_up, dense_down,
):
    parts = layer_call(
        tokens, mix_gain.reshape(1, 2048), w_query, w_key, w_value, w_outgate, w_ingate.T, w_forget.T,
        in_bias, forget_bias, cell_state, norm_state.reshape(96, 128), max_state.T, route_ids.T,
        w_mix_out, moe_gain.reshape(1, 2048), branch_gate.reshape(16, 128), route_weights.T,
        dense_gate.T, dense_up.T, dense_down,
        expert_gate.reshape(2048, 256), expert_up.reshape(2048, 256), expert_down.reshape(256, 2048),
    )
    layer_out, new_cell, new_norm, new_max = finish_call(*parts)
    return (layer_out, new_cell, new_norm.reshape(48, 2, 128), new_max.T)


def solution(mesh):
    in_specs = (
        P("ep", None),
        P(),
        P(None, "tp"),
        P(None, "tp"),
        P(None, "tp"),
        P(None, "tp"),
        P(None, "tp"),
        P(None, "tp"),
        P("tp"),
        P("tp"),
        P(),
        P("ep", "tp", None, None),
        P("ep", "tp", None),
        P("ep", "tp"),
        P(),
        P("ep", None),
        P("ep", None),
        P("ep", None, "tp"),
        P("ep", None, "tp"),
        P("ep", "tp", None),
        P(),
        P(None, ("ep", "tp")),
        P(None, ("ep", "tp")),
        P(("ep", "tp"), None),
    )
    out_specs = (P("ep", "tp"), P("ep", "tp", None, None), P("ep", "tp", None), P("ep", "tp"))
    return jax.shard_map(local, mesh=mesh, in_specs=in_specs, out_specs=out_specs, check_vma=False)
```

```python
import functools

import jax
import jax.numpy as jnp
from jax import lax
from jax.experimental import pallas as pl
from jax.experimental.pallas import tpu as pltpu
from jax.sharding import PartitionSpec as P

EPS = 1e-06
MESH = pl.DeviceIdType.MESH
F32 = jnp.float32
BF16 = jnp.bfloat16
NT = (((1,), (1,)), ((), ()))


def dot(a, b):
    return jnp.dot(a, b, preferred_element_type=F32)


def dot_nt(a, b):
    return lax.dot_general(a, b, NT, preferred_element_type=F32)


CHUNK = 12
N_CHUNK = 4


def split3(a):
    first = a.astype(BF16).astype(F32)
    rest = a - first
    second = rest.astype(BF16).astype(F32)
    return first, second, rest - second


def as_columns(rows):
    n, width = rows.shape
    wide = jnp.concatenate([rows, jnp.zeros((n, 128 - width), F32)], axis=1) if width < 128 else rows
    return jnp.concatenate([wide, jnp.zeros((128 - n, 128), F32)], axis=0).T


def slot_rows(ids):
    idf = ids.astype(F32)
    idc = as_columns(idf)
    before = lax.broadcasted_iota(jnp.int32, (48, 48), 0) < lax.broadcasted_iota(jnp.int32, (48, 48), 1)
    slots = []
    for ch in range(2):
        row = idf[ch : ch + 1, :]
        hits = jnp.where(idc[0:48, 0:1] == row, 1.0, 0.0) + jnp.where(idc[0:48, 1:2] == row, 1.0, 0.0)
        rank = jnp.sum(jnp.where(before, hits, 0.0), axis=0, keepdims=True)
        slots.append(row * 16.0 + rank)
    srow = jnp.concatenate(slots + [jnp.zeros((6, 48), F32)], axis=0)
    return jnp.concatenate([srow, jnp.zeros((8, 80), F32)], axis=1)


REL = [
    (0, 0), (1, 0), (3, 0), (0, 1), (0, 3),
    (1, 1), (1, 3), (3, 1), (3, 3), (2, 0), (0, 2),
    (2, 1), (2, 3), (1, 2), (3, 2),
    (2, 2),
]
IDX = {rel: i for i, rel in enumerate(REL)}
GROUPS = [(0, 5), (5, 6), (11, 4), (15, 1)]
ZP, ZM, YP, YM = (1, 0), (3, 0), (0, 1), (0, 3)
N_MSG = 160


def layer_kernel(
    tok_h, cgain_h, wq_h, wk_h, wv_h, wo_h, win_h, wf_h, inb_h, fb_h, cell_h, norm_h, max_h, ids_h,
    wmix_h, gain_h, bg_h, rw_h, gate_h, up_h, down_h, eg_h, eu_h, ed_h,
    out, cell, norm_o, max_o,
    inb, fb, tok, cgain, wts, win, wf, norm, mx, ids, normed, vs, vf, cb, qt, wt, num, wsem, csem, msem,
    ah, wmix, gain, bg, macc, rw, w, d, eg, eu, ed, meta, g, res, hid, xo, xp, xb, xs, xl, eh, el, ef, sb, rsr, rb, eret,
    ssem, rsem, lsem,
):
    me = lax.axis_index("ep")
    x = lax.axis_index("tp")
    c = lax.rem(me, 2)
    zy = lax.div(me, 2)
    y = lax.rem(zy, 4)
    z = lax.div(zy, 4)

    def dev(dz, dy, dx, pc):
        zz = lax.rem(z + dz, 4)
        yy = lax.rem(y + dy, 4)
        cc = 1 - c if pc else c
        return ((zz * 4 + yy) * 2 + cc, lax.rem(x + dx, 4))

    count = [0]
    sent = []

    class Msg:
        def __init__(self, src, dst, device):
            n = count[0]
            count[0] += 1
            self.copy = pltpu.make_async_remote_copy(
                src_ref=src, dst_ref=dst, send_sem=ssem.at[n], recv_sem=rsem.at[n], device_id=device, device_id_type=MESH
            )

        def start(self):
            self.copy.start()
            sent.append(self.copy)
            return self

        def arrived(self):
            self.copy.wait_recv()

    local = []

    def load(src, dst):
        cp = pltpu.make_async_copy(src, dst, lsem.at[len(local)])
        local.append(cp)
        cp.start()
        return cp

    barrier = pltpu.get_barrier_semaphore()
    peers = [dev(0, 0, 1, 0), dev(0, 0, 2, 0), dev(0, 0, 3, 0), dev(0, 0, 0, 1)]
    peers += [dev(dz, dy, 0, 0) for dz, dy in (ZP, ZM, YP, YM, (2, 0), (0, 2))]
    for peer in peers:
        pl.semaphore_signal(barrier, inc=1, device_id=peer, device_id_type=MESH)

    here = y * 4 + z
    cols = pl.ds(pl.multiple_of(x * 512, 512), 512)

    small = [
        pltpu.make_async_copy(src, dst, msem.at[i])
        for i, (src, dst) in enumerate(
            [(tok_h, tok), (cgain_h, cgain), (win_h, win), (wf_h, wf), (max_h, mx), (norm_h, norm), (ids_h, ids), (inb_h, inb), (fb_h, fb)]
        )
    ]
    for cp in small[0:2]:
        cp.start()
    wcp = [pltpu.make_async_copy(src, wts.at[i], wsem.at[i]) for i, src in enumerate([wq_h, wk_h, wv_h, wo_h])]
    wcp[0].start()
    for cp in small[2:]:
        cp.start()
    for cp in wcp[1:]:
        cp.start()

    def cin(i):
        s = pl.ds(i * CHUNK, CHUNK)
        return pltpu.make_async_copy(cell_h.at[s], cell.at[s], csem.at[i])

    for cp in small[0:2]:
        cp.wait()
    for i in range(N_CHUNK):
        cin(i).start()
    xf = tok[...].astype(F32)
    ms = jnp.mean(xf * xf, axis=-1, keepdims=True)
    normed[...] = (xf * lax.rsqrt(ms + EPS) * cgain[...]).astype(BF16)
    nb = normed[...]
    for cp in small[2:]:
        cp.wait()
    meta[here] = slot_rows(ids[...])
    in_pre = dot_nt(win[...], nb)
    fpre = dot_nt(wf[...], nb)
    hrow = lax.broadcasted_iota(jnp.int32, in_pre.shape, 0)
    in_pre = in_pre + jnp.where(hrow == 0, inb[0], inb[1])
    fpre = fpre + jnp.where(hrow == 0, fb[0], fb[1])
    log_f = jnp.minimum(fpre, 0.0) - jnp.log1p(jnp.exp(-jnp.abs(fpre)))
    lm = log_f + mx[...]
    new_max = jnp.maximum(lm, in_pre)
    max_o[...] = new_max
    carry = jnp.exp(lm - new_max)
    write = jnp.exp(in_pre - new_max)
    floor = jnp.exp(-new_max)
    rows = jnp.concatenate([carry, write, floor], axis=0)
    rows = jnp.concatenate([rows, jnp.zeros((6, 80), F32)], axis=1)
    rows = jnp.concatenate([rows, jnp.zeros((122, 128), F32)], axis=0)
    gcols = rows.T

    for cp in wcp:
        cp.wait()
    q = dot(nb, wts[0])
    k = dot(nb, wts[1]) * (128 ** (-0.5))
    v = dot(nb, wts[2])
    for h in range(2):
        v1, v2, _ = split3(v[:, h * 128 : (h + 1) * 128])
        vs[h] = jnp.concatenate([v1, v1, v2], axis=0).astype(BF16)
        vf[h] = v[:, h * 128 : (h + 1) * 128]
    og = jax.nn.sigmoid(dot(nb, wts[3]))

    cp_wmix = load(wmix_h, wmix)
    cp_gain = load(gain_h, gain)
    cp_bg = load(bg_h, bg)
    cp_rw = load(rw_h, rw)
    cp_gate = load(gate_h, w.at[0:64])
    cp_up = load(up_h, w.at[128:192])
    cp_down = load(down_h.at[:, cols], d.at[0:64])
    cp_ed = load(ed_h.at[:, cols], ed.at[0:256])
    cp_eg = load(eg_h, eg)
    cp_eu = load(eu_h, eu)

    pl.semaphore_wait(barrier, len(peers))
    w_p = [
        Msg(gate_h, w.at[64:128], dev(0, 0, 0, 1)).start(),
        Msg(up_h, w.at[192:256], dev(0, 0, 0, 1)).start(),
    ]
    down_p = [Msg(down_h.at[:, cols], d.at[64:128], dev(0, 0, 0, 1)).start()]
    down_x, ed_x = {}, {}

    def their(dx):
        return pl.ds(pl.multiple_of(lax.rem(x + dx, 4) * 512, 512), 512)

    def send_ed(dx):
        s = (4 - dx) % 4
        ed_x[s] = Msg(ed_h.at[:, their(dx)], ed.at[s * 256 : s * 256 + 256], dev(0, 0, dx, 0)).start()

    m_z = [Msg(meta.at[here], meta.at[here], dev(dz, 0, 0, 0)).start() for dz in (2, 1, 3)]

    denom = []
    pad = jnp.zeros((112, 128), F32)
    for h in range(2):
        ca = jnp.broadcast_to(gcols[0:48, h : h + 1], (48, 128))
        wr = jnp.broadcast_to(gcols[0:48, 2 + h : 3 + h], (48, 128))
        qh = q[:, h * 128 : (h + 1) * 128]
        written = wr * k[:, h * 128 : (h + 1) * 128]
        hs = pl.ds(h, 48, stride=2)
        nn = ca * norm[hs, :] + written
        norm_o[hs, :] = nn
        den = jnp.sum(qh * nn, axis=-1, keepdims=True)
        denom.append(jnp.maximum(jnp.abs(den), gcols[0:48, 4 + h : 5 + h]))
        cb[h] = ca
        vf[h] = jnp.sum(qh * written, axis=-1, keepdims=True) * vf[h]
        q1, q2, q3 = split3(qh)
        qt[h] = jnp.concatenate([q1, q2, q3, pad], axis=0).T[:, 0:144].astype(BF16)
        w1, w2, _ = split3(written)
        wt[h] = jnp.concatenate([w1, w2, w1, pad], axis=0).T[:, 0:144].astype(BF16)

    token = lax.rem(lax.broadcasted_iota(jnp.int32, (144, 128), 0), 48)

    def tokens_of(i):
        return [token == i * CHUNK + j for j in range(CHUNK)]

    def read_step(i, _):
        cin(i).wait()
        ones = jnp.concatenate([jnp.where(m, 1.0, 0.0) for m in tokens_of(i)], axis=1).astype(BF16)
        for h in range(2):
            qcols = dot(qt[h], ones)
            for j in range(CHUNK):
                b = i * CHUNK + j
                num[h, pl.ds(b, 1), :] = jnp.sum(
                    qcols[:, j * 128 : (j + 1) * 128] * cell[b, h], axis=0, keepdims=True
                )
        return 0

    def write_step(i, _):
        here = tokens_of(i)
        for h in range(2):
            vh = vs[h].astype(F32)
            vrows = jnp.concatenate([jnp.where(m, vh, 0.0) for m in here], axis=1).astype(BF16)
            outer = dot(wt[h], vrows)
            for j in range(CHUNK):
                b = i * CHUNK + j
                cell[b, h] = cb[h, pl.ds(b, 1), :] * cell[b, h] + outer[:, j * 128 : (j + 1) * 128]
        return 0

    lax.fori_loop(0, N_CHUNK, read_step, 0)
    for h in range(2):
        lanes = slice(h * 128, (h + 1) * 128)
        ah[x, :, lanes] = (og[:, lanes] * ((cb[h] * num[h] + vf[h]) / denom[h])).astype(BF16)

    heads = {}
    for dx in (2, 1, 3):
        heads[(4 - dx) % 4] = Msg(ah.at[x], ah.at[x], dev(0, 0, dx, 0)).start()

    cp_wmix.wait()
    cp_gain.wait()
    cp_bg.wait()

    def head_part(s, n):
        src = lax.rem(x + s, 4)
        rows = pl.ds(pl.multiple_of(src * 256, 256), 256)
        return dot(ah[src], wmix[rows, n * 512 : (n + 1) * 512])

    for n in range(4):
        s = slice(n * 512, (n + 1) * 512)
        macc[:, s] = tok[:, s].astype(F32) + head_part(0, n)
    for h in (1, 3):
        heads[h].arrived()
        for n in range(4):
            macc[:, n * 512 : (n + 1) * 512] += head_part(h, n)
    heads[2].arrived()
    sq = jnp.zeros((48, 1), F32)
    for n in range(4):
        s = slice(n * 512, (n + 1) * 512)
        r = (macc[:, s] + head_part(2, n)).astype(BF16)
        res[:, s] = r
        rf = r.astype(F32)
        sq = sq + jnp.sum(rf * rf, axis=-1, keepdims=True)
    inv = lax.rsqrt(sq * (1.0 / 2048.0) + EPS)
    for n in range(4):
        s = slice(n * 512, (n + 1) * 512)
        g[0, n] = (res[:, s].astype(F32) * inv * gain[:, s]).astype(BF16)

    def spread(rel, q0, nq, way):
        to = ((rel[0] - way[0]) % 4, (rel[1] - way[1]) % 4)
        q = pl.ds(q0, nq)
        return Msg(g.at[IDX[rel], q], g.at[IDX[to], q], dev(*way, 0, 0)).start()

    O = (0, 0)
    a_zp, a_zm = spread(O, 0, 2, ZP), spread(O, 0, 2, ZM)
    b_yp, b_ym = spread(O, 2, 2, YP), spread(O, 2, 2, YM)
    for m in m_z:
        m.arrived()
    col = pl.ds(y * 4, 4)
    m_y = [Msg(meta.at[col], meta.at[col], dev(0, dy, 0, 0)).start() for dy in (2, 1, 3)]
    a_yp, a_ym = spread(O, 0, 2, YP), spread(O, 0, 2, YM)
    b_zp, b_zm = spread(O, 2, 2, ZP), spread(O, 2, 2, ZM)

    for dx in (2, 1, 3):
        s = (4 - dx) % 4
        down_x[s] = Msg(down_h.at[:, their(dx)], d.at[s * 128 : s * 128 + 64], dev(0, 0, dx, 0)).start()
    for dx in (2, 1, 3):
        send_ed(dx)

    lax.fori_loop(0, N_CHUNK // 2, write_step, 0)

    gate_sum = jnp.zeros((48, 1), F32)
    gate_rows = bg[...].astype(F32)
    for n in range(4):
        rowsum = jnp.zeros((48, 128), F32)
        for i in range(4):
            rowsum = rowsum + g[0, n, :, i * 128 : (i + 1) * 128].astype(F32) * gate_rows[n * 4 + i : n * 4 + i + 1]
        gate_sum = gate_sum + jnp.sum(rowsum, axis=-1, keepdims=True)
    bw = jax.nn.sigmoid(gate_sum)
    cp_rw.wait()
    scol = as_columns(meta[here])
    rwc = as_columns(rw[...])

    a_zp.arrived()
    f_z0 = spread((3, 0), 0, 1, ZP)
    t_33, t_31 = spread((3, 0), 0, 2, YP), spread((3, 0), 0, 2, YM)
    a_zm.arrived()
    f_z1 = spread((1, 0), 1, 1, ZM)
    t_13, t_11 = spread((1, 0), 0, 2, YP), spread((1, 0), 0, 2, YM)
    b_yp.arrived()
    f_y2 = spread((0, 3), 2, 1, YP)
    u_33, u_13 = spread((0, 3), 2, 2, ZP), spread((0, 3), 2, 2, ZM)
    b_ym.arrived()
    f_y3 = spread((0, 1), 3, 1, YM)
    u_31, u_11 = spread((0, 1), 2, 2, ZP), spread((0, 1), 2, 2, ZM)
    a_yp.arrived()
    f_y0 = spread((0, 3), 0, 1, YP)
    a_ym.arrived()
    f_y1 = spread((0, 1), 1, 1, YM)
    b_zp.arrived()
    f_z2 = spread((3, 0), 2, 1, ZP)
    b_zm.arrived()
    f_z3 = spread((1, 0), 3, 1, ZM)

    def up_group(n):
        r0, nb = GROUPS[n]
        acc = None
        for q in range(4):
            part = dot_nt(g[r0 : r0 + nb, q].reshape(nb * 48, 512), w[:, q * 512 : (q + 1) * 512])
            acc = part if acc is None else acc + part
        ga, up = acc[:, 0:128], acc[:, 128:256]
        rows = pl.ds(r0 * 48, nb * 48)
        hid[rows, 0:128] = (ga * jax.nn.sigmoid(ga) * up).astype(BF16)
        out = {}
        for dx in (2, 1, 3):
            s = (4 - dx) % 4
            out[s] = Msg(hid.at[rows, 0:128], hid.at[rows, s * 128 : s * 128 + 128], dev(0, 0, dx, 0)).start()
        return out

    e_mine = (me * 16).astype(F32)
    e_other = ((zy * 2 + (1 - c)) * 16).astype(F32)

    def pick_group(n):
        r0, nb = GROUPS[n]
        lane8 = lax.broadcasted_iota(jnp.int32, (8, 48), 0).astype(F32)
        code = jnp.concatenate([lane8 + e_mine, lane8 + e_other], axis=0)
        for r in range(r0, r0 + nb):
            dz, dy = REL[r]
            m = meta[lax.rem(y + dy, 4) * 4 + lax.rem(z + dz, 4)]
            hit = jnp.where(m[0:1, 0:48] == code, 1.0, 0.0) + jnp.where(m[1:2, 0:48] == code, 1.0, 0.0)
            hit = hit.astype(BF16)
            for q in range(4):
                picked = dot(hit, g[r, q])
                s = slice(q * 512, (q + 1) * 512)
                if r == 15:
                    xl[0, :, s] = picked[0:8]
                    xl[1, :, s] = picked[8:16]
                else:
                    xo[r * 6 : r * 6 + 6, s] = picked[0:6]
                    xp[r * 6 : r * 6 + 6, s] = picked[8:14]

    xo[88:96, :] = jnp.zeros((8, 2048), F32)
    xp[88:96, :] = jnp.zeros((8, 2048), F32)

    def pass_rows(a, b):
        rows = slice(a, b)
        xs[rows] = xp[rows].astype(BF16)
        return Msg(xs.at[rows], xb.at[rows], dev(0, 0, 0, 1)).start()

    cp_down.wait()
    for s in (1, 2, 3):
        down_x[s].arrived()
        own = slice(s * 128, s * 128 + 64)
        down_p.append(Msg(d.at[own], d.at[s * 128 + 64 : s * 128 + 128], dev(0, 0, 0, 1)).start())

    cp_gate.wait()
    cp_up.wait()
    for m in w_p:
        m.arrived()
    hid_in = {}
    hid_in[0] = up_group(0)
    for m in m_y:
        m.arrived()
    pick_group(0)
    lax.fori_loop(N_CHUNK // 2, N_CHUNK, write_step, 0)

    f_z0.arrived()
    f_z1.arrived()
    t_23, t_21 = spread((2, 0), 0, 2, YP), spread((2, 0), 0, 2, YM)
    f_y2.arrived()
    f_y3.arrived()
    u_32, u_12 = spread((0, 2), 2, 2, ZP), spread((0, 2), 2, 2, ZM)
    t_33.arrived()
    h_32a = spread((3, 3), 0, 1, YP)
    t_31.arrived()
    h_32b = spread((3, 1), 1, 1, YM)
    t_13.arrived()
    h_12a = spread((1, 3), 0, 1, YP)
    t_11.arrived()
    h_12b = spread((1, 1), 1, 1, YM)
    u_33.arrived()
    h_23a = spread((3, 3), 2, 1, ZP)
    u_13.arrived()
    h_23b = spread((1, 3), 3, 1, ZM)
    u_31.arrived()
    h_21a = spread((3, 1), 2, 1, ZP)
    u_11.arrived()
    h_21b = spread((1, 1), 3, 1, ZM)
    for m in (f_y0, f_y1, f_z2, f_z3):
        m.arrived()

    reduced = {}

    def down_group(n):
        r0, nb = GROUPS[n]
        for m in hid_in[n].values():
            m.arrived()
        part = dot(hid[r0 * 48 : (r0 + nb) * 48, :], d[...])
        for i in range(nb):
            r = r0 + i
            blk = part[i * 48 : (i + 1) * 48].astype(BF16)
            if r == 0:
                rsr[0] = blk
            else:
                dz, dy = REL[r]
                sb[r] = blk
                back = IDX[((-dz) % 4, (-dy) % 4)]
                reduced[back] = Msg(sb.at[r], rsr.at[back], dev(dz, dy, 0, 0)).start()

    hid_in[1] = up_group(1)

    t_23.arrived()
    l_22a = spread((2, 3), 0, 1, YP)
    t_21.arrived()
    l_22b = spread((2, 1), 1, 1, YM)
    u_32.arrived()
    l_22c = spread((3, 2), 2, 1, ZP)
    u_12.arrived()
    l_22d = spread((1, 2), 3, 1, ZM)

    pick_group(1)
    first_rows = pass_rows(0, 48)
    for m in (h_32a, h_32b, h_12a, h_12b, h_23a, h_23b, h_21a, h_21b):
        m.arrived()
    hid_in[2] = up_group(2)
    pick_group(2)
    second_rows = pass_rows(48, 96)

    cp_eg.wait()
    cp_eu.wait()

    def expert_up(ref, rows_in):
        ga = dot(rows_in, eg[...])
        up = dot(rows_in, eu[...])
        ref[:, 0:256] = (ga * jax.nn.sigmoid(ga) * up).astype(BF16)
        out = []
        for dx in (2, 1, 3):
            s = (4 - dx) % 4
            out.append(Msg(ref.at[:, 0:256], ref.at[:, s * 256 : s * 256 + 256], dev(0, 0, dx, 0)).start())
        return out

    first_rows.arrived()
    eh_in = expert_up(eh, jnp.concatenate([xo[0:48].astype(BF16), xb[0:48]], axis=0))
    for m in down_p:
        m.arrived()
    down_group(0)

    for m in (l_22a, l_22b, l_22c, l_22d):
        m.arrived()
    pick_group(3)
    last_rows = Msg(xl.at[1], xl.at[2], dev(0, 0, 0, 1)).start()
    hid_in[3] = up_group(3)
    down_group(1)

    second_rows.arrived()
    el_in = expert_up(el, jnp.concatenate([xo[48:96].astype(BF16), xb[48:96]], axis=0))
    down_group(2)
    last_rows.arrived()
    ef_in = expert_up(ef, jnp.concatenate([xl[0], xl[2]], axis=0).astype(BF16))
    down_group(3)

    cp_ed.wait()
    for m in ed_x.values():
        m.arrived()
    returned = []

    def give_back(half, r, eo):
        blk = jnp.concatenate([eo[:, 0:256], eo[:, 256:512]], axis=0).astype(BF16)
        if r == 0 and half == 0:
            eret[me] = blk
        else:
            dz, dy = REL[r]
            rb[half, r] = blk
            returned.append(Msg(rb.at[half, r], eret.at[me], dev(dz, dy, 0, half)).start())

    def results(ref):
        return jnp.concatenate([dot(ref[...], ed[...]), jnp.zeros((8, 512), F32)], axis=0)

    for m in eh_in:
        m.arrived()
    eo = results(eh)
    for r in range(7, -1, -1):
        for half in range(2):
            give_back(half, r, eo[half * 48 + r * 6 : half * 48 + r * 6 + 8])
    for m in el_in:
        m.arrived()
    eo = results(el)
    for r in range(14, 7, -1):
        for half in range(2):
            give_back(half, r, eo[half * 48 + (r - 8) * 6 : half * 48 + (r - 8) * 6 + 8])
    for m in ef_in:
        m.arrived()
    eo = dot(ef[...], ed[...])
    for half in range(2):
        give_back(half, 15, eo[half * 8 : half * 8 + 8])

    lane = lax.broadcasted_iota(jnp.int32, (48, 512), 1).astype(F32)
    sel = jnp.concatenate(
        [jnp.where(lane == scol[0:48, ch : ch + 1] + float(hf * 8), 1.0, 0.0) for hf in range(2) for ch in range(2)], axis=0
    ).astype(BF16)
    total = rsr[0].astype(F32)
    for r in range(1, 16):
        reduced[r].arrived()
        total = total + rsr[r].astype(F32)
    base = res[:, cols].astype(F32) + bw * total
    for m in returned:
        m.arrived()
    got = dot(sel, eret[...].reshape(512, 256))
    for hf in range(2):
        s = slice(hf * 256, hf * 256 + 256)
        first, second = got[hf * 96 : hf * 96 + 48], got[hf * 96 + 48 : hf * 96 + 96]
        out[:, s] = (base[:, s] + first * rwc[0:48, 0:1] + second * rwc[0:48, 1:2]).astype(BF16)

    for cp in sent:
        cp.wait_send()


def layer_call(*args):
    vm = pl.BlockSpec(memory_space=pltpu.VMEM)
    args = [pltpu.with_memory_space_constraint(a, pltpu.HBM) for a in args]
    return pl.pallas_call(
        layer_kernel,
        out_shape=(
            jax.ShapeDtypeStruct((48, 512), BF16),
            jax.ShapeDtypeStruct((48, 2, 128, 128), F32),
            jax.ShapeDtypeStruct((96, 128), F32),
            jax.ShapeDtypeStruct((2, 48), F32),
        ),
        in_specs=[pl.BlockSpec(memory_space=pltpu.HBM)] * 24,
        out_specs=(vm, vm, vm, vm),
        scratch_shapes=[
            pltpu.SMEM((2,), F32),
            pltpu.SMEM((2,), F32),
            pltpu.VMEM((48, 2048), BF16),
            pltpu.VMEM((1, 2048), F32),
            pltpu.VMEM((4, 2048, 256), BF16),
            pltpu.VMEM((2, 2048), BF16),
            pltpu.VMEM((2, 2048), BF16),
            pltpu.VMEM((96, 128), F32),
            pltpu.VMEM((2, 48), F32),
            pltpu.VMEM((2, 48), jnp.int32),
            pltpu.VMEM((48, 2048), BF16),
            pltpu.VMEM((2, 144, 128), BF16),
            pltpu.VMEM((2, 48, 128), F32),
            pltpu.VMEM((2, 48, 128), F32),
            pltpu.VMEM((2, 128, 144), BF16),
            pltpu.VMEM((2, 128, 144), BF16),
            pltpu.VMEM((2, 48, 128), F32),
            pltpu.SemaphoreType.DMA((4,)),
            pltpu.SemaphoreType.DMA((N_CHUNK,)),
            pltpu.SemaphoreType.DMA((9,)),
            pltpu.VMEM((4, 48, 256), BF16),
            pltpu.VMEM((1024, 2048), BF16),
            pltpu.VMEM((1, 2048), F32),
            pltpu.VMEM((16, 128), BF16),
            pltpu.VMEM((48, 2048), F32),
            pltpu.VMEM((2, 48), F32),
            pltpu.VMEM((256, 2048), BF16),
            pltpu.VMEM((512, 512), BF16),
            pltpu.VMEM((2048, 256), BF16),
            pltpu.VMEM((2048, 256), BF16),
            pltpu.VMEM((1024, 512), BF16),
            pltpu.VMEM((16, 8, 128), F32),
            pltpu.VMEM((16, 4, 48, 512), BF16),
            pltpu.VMEM((48, 2048), BF16),
            pltpu.VMEM((768, 512), BF16),
            pltpu.VMEM((96, 2048), F32),
            pltpu.VMEM((96, 2048), F32),
            pltpu.VMEM((96, 2048), BF16),
            pltpu.VMEM((96, 2048), BF16),
            pltpu.VMEM((3, 8, 2048), F32),
            pltpu.VMEM((96, 1024), BF16),
            pltpu.VMEM((96, 1024), BF16),
            pltpu.VMEM((16, 1024), BF16),
            pltpu.VMEM((16, 48, 512), BF16),
            pltpu.VMEM((16, 48, 512), BF16),
            pltpu.VMEM((2, 16, 16, 256), BF16),
            pltpu.VMEM((32, 16, 256), BF16),
            pltpu.SemaphoreType.DMA((N_MSG,)),
            pltpu.SemaphoreType.DMA((N_MSG,)),
            pltpu.SemaphoreType.DMA((16,)),
        ],
        compiler_params=pltpu.CompilerParams(vmem_limit_bytes=44 * 2**20, collective_id=0, has_side_effects=True),
        name="layer",
    )(*args)


def finish_kernel(lay, cell, norm, mx, lay_o, cell_o, norm_o, max_o, sem):
    copies = [
        pltpu.make_async_copy(cell.at[12 * i : 12 * i + 12], cell_o.at[12 * i : 12 * i + 12], sem.at[i]) for i in range(4)
    ]
    copies.append(pltpu.make_async_copy(lay, lay_o, sem.at[4]))
    copies.append(pltpu.make_async_copy(norm, norm_o, sem.at[5]))
    copies.append(pltpu.make_async_copy(mx, max_o, sem.at[6]))
    for cp in copies:
        cp.start()
    for cp in copies:
        cp.wait()


def finish_call(*args):
    any_ = pl.BlockSpec(memory_space=pl.ANY)
    vm = pl.BlockSpec(memory_space=pltpu.VMEM)
    return pl.pallas_call(
        finish_kernel,
        out_shape=tuple(jax.ShapeDtypeStruct(a.shape, a.dtype) for a in args),
        in_specs=[vm] * 4,
        out_specs=[any_] * 4,
        scratch_shapes=[pltpu.SemaphoreType.DMA((7,))],
        compiler_params=pltpu.CompilerParams(vmem_limit_bytes=16 * 2**20),
        name="finish",
    )(*[pltpu.with_memory_space_constraint(a, pltpu.VMEM) for a in args])


def local(
    tokens, mix_gain, w_query, w_key, w_value, w_outgate, w_ingate, w_forget, in_bias, forget_bias, w_mix_out,
    cell_state, norm_state, max_state, moe_gain, route_ids, route_weights, expert_gate, expert_up, expert_down,
    branch_gate, dense_gate, dense_up, dense_down,
):
    parts = layer_call(
        tokens, mix_gain.reshape(1, 2048), w_query, w_key, w_value, w_outgate, w_ingate.T, w_forget.T,
        in_bias, forget_bias, cell_state, norm_state.reshape(96, 128), max_state.T, route_ids.T,
        w_mix_out, moe_gain.reshape(1, 2048), branch_gate.reshape(16, 128), route_weights.T,
        dense_gate.T, dense_up.T, dense_down,
        expert_gate.reshape(2048, 256), expert_up.reshape(2048, 256), expert_down.reshape(256, 2048),
    )
    layer_out, new_cell, new_norm, new_max = finish_call(*parts)
    return (layer_out, new_cell, new_norm.reshape(48, 2, 128), new_max.T)


def solution(mesh):
    in_specs = (
        P("ep", None),
        P(),
        P(None, "tp"),
        P(None, "tp"),
        P(None, "tp"),
        P(None, "tp"),
        P(None, "tp"),
        P(None, "tp"),
        P("tp"),
        P("tp"),
        P(),
        P("ep", "tp", None, None),
        P("ep", "tp", None),
        P("ep", "tp"),
        P(),
        P("ep", None),
        P("ep", None),
        P("ep", None, "tp"),
        P("ep", None, "tp"),
        P("ep", "tp", None),
        P(),
        P(None, ("ep", "tp")),
        P(None, ("ep", "tp")),
        P(("ep", "tp"), None),
    )
    out_specs = (P("ep", "tp"), P("ep", "tp", None, None), P("ep", "tp", None), P("ep", "tp"))
    return jax.shard_map(local, mesh=mesh, in_specs=in_specs, out_specs=out_specs, check_vma=False)
```

```python
import functools

import jax
import jax.numpy as jnp
from jax import lax
from jax.experimental import pallas as pl
from jax.experimental.pallas import tpu as pltpu
from jax.sharding import PartitionSpec as P

EPS = 1e-06
MESH = pl.DeviceIdType.MESH
F32 = jnp.float32
BF16 = jnp.bfloat16
NT = (((1,), (1,)), ((), ()))


def dot(a, b):
    return jnp.dot(a, b, preferred_element_type=F32)


def dot_nt(a, b):
    return lax.dot_general(a, b, NT, preferred_element_type=F32)


CHUNK = 12
N_CHUNK = 4


def split3(a):
    first = a.astype(BF16).astype(F32)
    rest = a - first
    second = rest.astype(BF16).astype(F32)
    return first, second, rest - second


def as_columns(rows):
    n, width = rows.shape
    wide = jnp.concatenate([rows, jnp.zeros((n, 128 - width), F32)], axis=1) if width < 128 else rows
    return jnp.concatenate([wide, jnp.zeros((128 - n, 128), F32)], axis=0).T


def slot_rows(ids):
    idf = ids.astype(F32)
    idc = as_columns(idf)
    before = lax.broadcasted_iota(jnp.int32, (48, 48), 0) < lax.broadcasted_iota(jnp.int32, (48, 48), 1)
    slots = []
    for ch in range(2):
        row = idf[ch : ch + 1, :]
        hits = jnp.where(idc[0:48, 0:1] == row, 1.0, 0.0) + jnp.where(idc[0:48, 1:2] == row, 1.0, 0.0)
        rank = jnp.sum(jnp.where(before, hits, 0.0), axis=0, keepdims=True)
        slots.append(row * 16.0 + rank)
    srow = jnp.concatenate(slots + [jnp.zeros((6, 48), F32)], axis=0)
    return jnp.concatenate([srow, jnp.zeros((8, 80), F32)], axis=1)


REL = [
    (0, 0), (1, 0), (3, 0), (0, 1), (0, 3),
    (1, 1), (1, 3), (3, 1), (3, 3), (2, 0), (0, 2),
    (2, 1), (2, 3), (1, 2), (3, 2),
    (2, 2),
]
IDX = {rel: i for i, rel in enumerate(REL)}
GROUPS = [(0, 5), (5, 6), (11, 4), (15, 1)]
ZP, ZM, YP, YM = (1, 0), (3, 0), (0, 1), (0, 3)
N_MSG = 160


def layer_kernel(
    tok_h, cgain_h, wq_h, wk_h, wv_h, wo_h, win_h, wf_h, inb_h, fb_h, cell_h, norm_h, max_h, ids_h,
    wmix_h, gain_h, bg_h, rw_h, gate_h, up_h, down_h, eg_h, eu_h, ed_h,
    out, cell, norm_o, max_o,
    inb, fb, tok, cgain, wts, win, wf, norm, mx, ids, normed, vs, vf, cb, qt, wt, num, wsem, csem, msem,
    ah, wmix, gain, bg, macc, rw, w, d, eg, eu, ed, meta, g, res, hid, xo, xp, xb, xs, xl, eh, el, sb, rsr, rb, eret,
    ssem, rsem, lsem,
):
    me = lax.axis_index("ep")
    x = lax.axis_index("tp")
    c = lax.rem(me, 2)
    zy = lax.div(me, 2)
    y = lax.rem(zy, 4)
    z = lax.div(zy, 4)

    def dev(dz, dy, dx, pc):
        zz = lax.rem(z + dz, 4)
        yy = lax.rem(y + dy, 4)
        cc = 1 - c if pc else c
        return ((zz * 4 + yy) * 2 + cc, lax.rem(x + dx, 4))

    count = [0]
    sent = []

    class Msg:
        def __init__(self, src, dst, device):
            n = count[0]
            count[0] += 1
            self.copy = pltpu.make_async_remote_copy(
                src_ref=src, dst_ref=dst, send_sem=ssem.at[n], recv_sem=rsem.at[n], device_id=device, device_id_type=MESH
            )

        def start(self):
            self.copy.start()
            sent.append(self.copy)
            return self

        def arrived(self):
            self.copy.wait_recv()

    local = []

    def load(src, dst):
        cp = pltpu.make_async_copy(src, dst, lsem.at[len(local)])
        local.append(cp)
        cp.start()
        return cp

    barrier = pltpu.get_barrier_semaphore()
    peers = [dev(0, 0, 1, 0), dev(0, 0, 2, 0), dev(0, 0, 3, 0), dev(0, 0, 0, 1)]
    peers += [dev(dz, dy, 0, 0) for dz, dy in (ZP, ZM, YP, YM, (2, 0), (0, 2))]
    here = y * 4 + z
    cols = pl.ds(pl.multiple_of(x * 512, 512), 512)

    small = [
        pltpu.make_async_copy(src, dst, msem.at[i])
        for i, (src, dst) in enumerate(
            [(tok_h, tok), (cgain_h, cgain), (win_h, win), (wf_h, wf), (max_h, mx), (norm_h, norm), (ids_h, ids), (inb_h, inb), (fb_h, fb)]
        )
    ]
    for cp in small[0:2]:
        cp.start()
    wcp = [pltpu.make_async_copy(src, wts.at[i], wsem.at[i]) for i, src in enumerate([wq_h, wk_h, wv_h, wo_h])]
    wcp[0].start()
    for cp in small[2:]:
        cp.start()
    for cp in wcp[1:]:
        cp.start()

    def cin(i):
        s = pl.ds(i * CHUNK, CHUNK)
        return pltpu.make_async_copy(cell_h.at[s], cell.at[s], csem.at[i])

    for peer in peers:
        pl.semaphore_signal(barrier, inc=1, device_id=peer, device_id_type=MESH)
    for cp in small[0:2]:
        cp.wait()
    for i in range(N_CHUNK):
        cin(i).start()
    xf = tok[...].astype(F32)
    ms = jnp.mean(xf * xf, axis=-1, keepdims=True)
    normed[...] = (xf * lax.rsqrt(ms + EPS) * cgain[...]).astype(BF16)
    nb = normed[...]
    for cp in small[2:]:
        cp.wait()
    meta[here] = slot_rows(ids[...])
    in_pre = dot_nt(win[...], nb)
    fpre = dot_nt(wf[...], nb)
    hrow = lax.broadcasted_iota(jnp.int32, in_pre.shape, 0)
    in_pre = in_pre + jnp.where(hrow == 0, inb[0], inb[1])
    fpre = fpre + jnp.where(hrow == 0, fb[0], fb[1])
    log_f = jnp.minimum(fpre, 0.0) - jnp.log1p(jnp.exp(-jnp.abs(fpre)))
    lm = log_f + mx[...]
    new_max = jnp.maximum(lm, in_pre)
    max_o[...] = new_max
    carry = jnp.exp(lm - new_max)
    write = jnp.exp(in_pre - new_max)
    floor = jnp.exp(-new_max)
    rows = jnp.concatenate([carry, write, floor], axis=0)
    rows = jnp.concatenate([rows, jnp.zeros((6, 80), F32)], axis=1)
    rows = jnp.concatenate([rows, jnp.zeros((122, 128), F32)], axis=0)
    gcols = rows.T

    for cp in wcp:
        cp.wait()
    q = dot(nb, wts[0])
    k = dot(nb, wts[1]) * (128 ** (-0.5))
    v = dot(nb, wts[2])
    for h in range(2):
        v1, v2, _ = split3(v[:, h * 128 : (h + 1) * 128])
        vs[h] = jnp.concatenate([v1, v1, v2], axis=0).astype(BF16)
        vf[h] = v[:, h * 128 : (h + 1) * 128]
    og = jax.nn.sigmoid(dot(nb, wts[3]))

    cp_wmix = load(wmix_h, wmix)
    cp_gain = load(gain_h, gain)
    cp_bg = load(bg_h, bg)
    cp_rw = load(rw_h, rw)
    cp_gate = load(gate_h, w.at[0:64])
    cp_up = load(up_h, w.at[128:192])
    cp_down = load(down_h.at[:, cols], d.at[0:64])
    cp_ed = load(ed_h.at[:, cols], ed.at[0:256])
    cp_eg = load(eg_h, eg)
    cp_eu = load(eu_h, eu)

    pl.semaphore_wait(barrier, len(peers))
    w_p = [
        Msg(gate_h, w.at[64:128], dev(0, 0, 0, 1)).start(),
        Msg(up_h, w.at[192:256], dev(0, 0, 0, 1)).start(),
    ]
    down_p = [Msg(down_h.at[:, cols], d.at[64:128], dev(0, 0, 0, 1)).start()]
    down_x, ed_x = {}, {}

    def their(dx):
        return pl.ds(pl.multiple_of(lax.rem(x + dx, 4) * 512, 512), 512)

    def send_ed(dx):
        s = (4 - dx) % 4
        ed_x[s] = Msg(ed_h.at[:, their(dx)], ed.at[s * 256 : s * 256 + 256], dev(0, 0, dx, 0)).start()

    m_z = [Msg(meta.at[here], meta.at[here], dev(dz, 0, 0, 0)).start() for dz in (2, 1, 3)]

    denom = []
    pad = jnp.zeros((112, 128), F32)
    for h in range(2):
        ca = jnp.broadcast_to(gcols[0:48, h : h + 1], (48, 128))
        wr = jnp.broadcast_to(gcols[0:48, 2 + h : 3 + h], (48, 128))
        qh = q[:, h * 128 : (h + 1) * 128]
        written = wr * k[:, h * 128 : (h + 1) * 128]
        hs = pl.ds(h, 48, stride=2)
        nn = ca * norm[hs, :] + written
        norm_o[hs, :] = nn
        den = jnp.sum(qh * nn, axis=-1, keepdims=True)
        denom.append(jnp.maximum(jnp.abs(den), gcols[0:48, 4 + h : 5 + h]))
        cb[h] = ca
        vf[h] = jnp.sum(qh * written, axis=-1, keepdims=True) * vf[h]
        q1, q2, q3 = split3(qh)
        qt[h] = jnp.concatenate([q1, q2, q3, pad], axis=0).T[:, 0:144].astype(BF16)
        w1, w2, _ = split3(written)
        wt[h] = jnp.concatenate([w1, w2, w1, pad], axis=0).T[:, 0:144].astype(BF16)

    token = lax.rem(lax.broadcasted_iota(jnp.int32, (144, 128), 0), 48)

    def tokens_of(i):
        return [token == i * CHUNK + j for j in range(CHUNK)]

    def read_step(i, _):
        cin(i).wait()
        ones = jnp.concatenate([jnp.where(m, 1.0, 0.0) for m in tokens_of(i)], axis=1).astype(BF16)
        for h in range(2):
            qcols = dot(qt[h], ones)
            for j in range(CHUNK):
                b = i * CHUNK + j
                num[h, pl.ds(b, 1), :] = jnp.sum(
                    qcols[:, j * 128 : (j + 1) * 128] * cell[b, h], axis=0, keepdims=True
                )
        return 0

    def write_step(i, _):
        here = tokens_of(i)
        for h in range(2):
            vh = vs[h].astype(F32)
            vrows = jnp.concatenate([jnp.where(m, vh, 0.0) for m in here], axis=1).astype(BF16)
            outer = dot(wt[h], vrows)
            for j in range(CHUNK):
                b = i * CHUNK + j
                cell[b, h] = cb[h, pl.ds(b, 1), :] * cell[b, h] + outer[:, j * 128 : (j + 1) * 128]
        return 0

    lax.fori_loop(0, N_CHUNK, read_step, 0)
    for h in range(2):
        lanes = slice(h * 128, (h + 1) * 128)
        ah[x, :, lanes] = (og[:, lanes] * ((cb[h] * num[h] + vf[h]) / denom[h])).astype(BF16)

    heads = {}
    for dx in (2, 1, 3):
        heads[(4 - dx) % 4] = Msg(ah.at[x], ah.at[x], dev(0, 0, dx, 0)).start()

    cp_wmix.wait()
    cp_gain.wait()
    cp_bg.wait()

    def head_part(s, n):
        src = lax.rem(x + s, 4)
        rows = pl.ds(pl.multiple_of(src * 256, 256), 256)
        return dot(ah[src], wmix[rows, n * 512 : (n + 1) * 512])

    for n in range(4):
        s = slice(n * 512, (n + 1) * 512)
        macc[:, s] = tok[:, s].astype(F32) + head_part(0, n)
    for h in (1, 3):
        heads[h].arrived()
        for n in range(4):
            macc[:, n * 512 : (n + 1) * 512] += head_part(h, n)
    heads[2].arrived()
    sq = jnp.zeros((48, 1), F32)
    for n in range(4):
        s = slice(n * 512, (n + 1) * 512)
        r = (macc[:, s] + head_part(2, n)).astype(BF16)
        res[:, s] = r
        rf = r.astype(F32)
        sq = sq + jnp.sum(rf * rf, axis=-1, keepdims=True)
    inv = lax.rsqrt(sq * (1.0 / 2048.0) + EPS)
    for n in range(4):
        s = slice(n * 512, (n + 1) * 512)
        g[0, n] = (res[:, s].astype(F32) * inv * gain[:, s]).astype(BF16)

    def spread(rel, q0, nq, way):
        to = ((rel[0] - way[0]) % 4, (rel[1] - way[1]) % 4)
        q = pl.ds(q0, nq)
        return Msg(g.at[IDX[rel], q], g.at[IDX[to], q], dev(*way, 0, 0)).start()

    O = (0, 0)
    a_zp, a_zm = spread(O, 0, 2, ZP), spread(O, 0, 2, ZM)
    b_yp, b_ym = spread(O, 2, 2, YP), spread(O, 2, 2, YM)
    for m in m_z:
        m.arrived()
    col = pl.ds(y * 4, 4)
    m_y = [Msg(meta.at[col], meta.at[col], dev(0, dy, 0, 0)).start() for dy in (2, 1, 3)]
    a_yp, a_ym = spread(O, 0, 2, YP), spread(O, 0, 2, YM)
    b_zp, b_zm = spread(O, 2, 2, ZP), spread(O, 2, 2, ZM)

    for dx in (2, 1, 3):
        s = (4 - dx) % 4
        down_x[s] = Msg(down_h.at[:, their(dx)], d.at[s * 128 : s * 128 + 64], dev(0, 0, dx, 0)).start()
    for dx in (2, 1, 3):
        send_ed(dx)

    lax.fori_loop(0, N_CHUNK // 2, write_step, 0)

    gate_sum = jnp.zeros((48, 1), F32)
    gate_rows = bg[...].astype(F32)
    for n in range(4):
        rowsum = jnp.zeros((48, 128), F32)
        for i in range(4):
            rowsum = rowsum + g[0, n, :, i * 128 : (i + 1) * 128].astype(F32) * gate_rows[n * 4 + i : n * 4 + i + 1]
        gate_sum = gate_sum + jnp.sum(rowsum, axis=-1, keepdims=True)
    bw = jax.nn.sigmoid(gate_sum)
    cp_rw.wait()
    scol = as_columns(meta[here])
    rwc = as_columns(rw[...])

    a_zp.arrived()
    f_z0 = spread((3, 0), 0, 1, ZP)
    t_33, t_31 = spread((3, 0), 0, 2, YP), spread((3, 0), 0, 2, YM)
    a_zm.arrived()
    f_z1 = spread((1, 0), 1, 1, ZM)
    t_13, t_11 = spread((1, 0), 0, 2, YP), spread((1, 0), 0, 2, YM)
    b_yp.arrived()
    f_y2 = spread((0, 3), 2, 1, YP)
    u_33, u_13 = spread((0, 3), 2, 2, ZP), spread((0, 3), 2, 2, ZM)
    b_ym.arrived()
    f_y3 = spread((0, 1), 3, 1, YM)
    u_31, u_11 = spread((0, 1), 2, 2, ZP), spread((0, 1), 2, 2, ZM)
    a_yp.arrived()
    f_y0 = spread((0, 3), 0, 1, YP)
    a_ym.arrived()
    f_y1 = spread((0, 1), 1, 1, YM)
    b_zp.arrived()
    f_z2 = spread((3, 0), 2, 1, ZP)
    b_zm.arrived()
    f_z3 = spread((1, 0), 3, 1, ZM)

    def up_group(n):
        r0, nb = GROUPS[n]
        acc = None
        for q in range(4):
            part = dot_nt(g[r0 : r0 + nb, q].reshape(nb * 48, 512), w[:, q * 512 : (q + 1) * 512])
            acc = part if acc is None else acc + part
        ga, up = acc[:, 0:128], acc[:, 128:256]
        rows = pl.ds(r0 * 48, nb * 48)
        hid[rows, 0:128] = (ga * jax.nn.sigmoid(ga) * up).astype(BF16)
        out = {}
        for dx in (2, 1, 3):
            s = (4 - dx) % 4
            out[s] = Msg(hid.at[rows, 0:128], hid.at[rows, s * 128 : s * 128 + 128], dev(0, 0, dx, 0)).start()
        return out

    e_mine = (me * 16).astype(F32)
    e_other = ((zy * 2 + (1 - c)) * 16).astype(F32)

    def pick_group(n):
        r0, nb = GROUPS[n]
        lane8 = lax.broadcasted_iota(jnp.int32, (8, 48), 0).astype(F32)
        code = jnp.concatenate([lane8 + e_mine, lane8 + e_other], axis=0)
        for r in range(r0, r0 + nb):
            dz, dy = REL[r]
            m = meta[lax.rem(y + dy, 4) * 4 + lax.rem(z + dz, 4)]
            hit = jnp.where(m[0:1, 0:48] == code, 1.0, 0.0) + jnp.where(m[1:2, 0:48] == code, 1.0, 0.0)
            hit = hit.astype(BF16)
            for q in range(4):
                picked = dot(hit, g[r, q])
                s = slice(q * 512, (q + 1) * 512)
                if r == 15:
                    xl[0, :, s] = picked[0:8]
                    xl[1, :, s] = picked[8:16]
                else:
                    xo[r * 6 : r * 6 + 6, s] = picked[0:6]
                    xp[r * 6 : r * 6 + 6, s] = picked[8:14]

    xo[88:96, :] = jnp.zeros((8, 2048), F32)
    xp[88:96, :] = jnp.zeros((8, 2048), F32)

    def pass_rows(a, b):
        rows = slice(a, b)
        xs[rows] = xp[rows].astype(BF16)
        return Msg(xs.at[rows], xb.at[rows], dev(0, 0, 0, 1)).start()

    cp_down.wait()
    for s in (1, 2, 3):
        down_x[s].arrived()
        own = slice(s * 128, s * 128 + 64)
        down_p.append(Msg(d.at[own], d.at[s * 128 + 64 : s * 128 + 128], dev(0, 0, 0, 1)).start())

    cp_gate.wait()
    cp_up.wait()
    for m in w_p:
        m.arrived()
    hid_in = {}
    hid_in[0] = up_group(0)
    for m in m_y:
        m.arrived()
    pick_group(0)
    lax.fori_loop(N_CHUNK // 2, N_CHUNK, write_step, 0)

    f_z0.arrived()
    f_z1.arrived()
    t_23, t_21 = spread((2, 0), 0, 2, YP), spread((2, 0), 0, 2, YM)
    f_y2.arrived()
    f_y3.arrived()
    u_32, u_12 = spread((0, 2), 2, 2, ZP), spread((0, 2), 2, 2, ZM)
    t_33.arrived()
    h_32a = spread((3, 3), 0, 1, YP)
    t_31.arrived()
    h_32b = spread((3, 1), 1, 1, YM)
    t_13.arrived()
    h_12a = spread((1, 3), 0, 1, YP)
    t_11.arrived()
    h_12b = spread((1, 1), 1, 1, YM)
    u_33.arrived()
    h_23a = spread((3, 3), 2, 1, ZP)
    u_13.arrived()
    h_23b = spread((1, 3), 3, 1, ZM)
    u_31.arrived()
    h_21a = spread((3, 1), 2, 1, ZP)
    u_11.arrived()
    h_21b = spread((1, 1), 3, 1, ZM)
    for m in (f_y0, f_y1, f_z2, f_z3):
        m.arrived()

    reduced = {}

    def down_group(n):
        r0, nb = GROUPS[n]
        for m in hid_in[n].values():
            m.arrived()
        part = dot(hid[r0 * 48 : (r0 + nb) * 48, :], d[...])
        for i in range(nb):
            r = r0 + i
            blk = part[i * 48 : (i + 1) * 48].astype(BF16)
            if r == 0:
                rsr[0] = blk
            else:
                dz, dy = REL[r]
                sb[r] = blk
                back = IDX[((-dz) % 4, (-dy) % 4)]
                reduced[back] = Msg(sb.at[r], rsr.at[back], dev(dz, dy, 0, 0)).start()

    hid_in[1] = up_group(1)

    pick_group(1)
    first_rows = pass_rows(0, 48)

    t_23.arrived()
    l_22a = spread((2, 3), 0, 1, YP)
    t_21.arrived()
    l_22b = spread((2, 1), 1, 1, YM)
    u_32.arrived()
    l_22c = spread((3, 2), 2, 1, ZP)
    u_12.arrived()
    l_22d = spread((1, 2), 3, 1, ZM)

    for m in down_p:
        m.arrived()
    down_group(0)
    for m in (h_32a, h_32b, h_12a, h_12b, h_23a, h_23b, h_21a, h_21b):
        m.arrived()
    hid_in[2] = up_group(2)
    pick_group(2)
    second_rows = pass_rows(48, 96)

    cp_eg.wait()
    cp_eu.wait()

    def expert_up(ref, rows_in):
        ga = dot(rows_in, eg[...])
        up = dot(rows_in, eu[...])
        ref[:, 0:256] = (ga * jax.nn.sigmoid(ga) * up).astype(BF16)
        out = []
        for dx in (2, 1, 3):
            s = (4 - dx) % 4
            out.append(Msg(ref.at[:, 0:256], ref.at[:, s * 256 : s * 256 + 256], dev(0, 0, dx, 0)).start())
        return out

    first_rows.arrived()
    eh_in = expert_up(eh, jnp.concatenate([xo[0:48].astype(BF16), xb[0:48]], axis=0))

    for m in (l_22a, l_22b, l_22c, l_22d):
        m.arrived()
    pick_group(3)
    last_rows = Msg(xl.at[1], xl.at[2], dev(0, 0, 0, 1)).start()
    hid_in[3] = up_group(3)
    down_group(1)
    second_rows.arrived()
    el_in = expert_up(el.at[0:96], jnp.concatenate([xo[48:96].astype(BF16), xb[48:96]], axis=0))
    down_group(2)
    last_rows.arrived()
    el_in += expert_up(el.at[96:112], jnp.concatenate([xl[0], xl[2]], axis=0).astype(BF16))
    down_group(3)

    cp_ed.wait()
    for m in ed_x.values():
        m.arrived()
    returned = []

    def give_back(half, r, eo):
        blk = jnp.concatenate([eo[:, 0:256], eo[:, 256:512]], axis=0).astype(BF16)
        if r == 0 and half == 0:
            eret[me] = blk
        else:
            dz, dy = REL[r]
            rb[half, r] = blk
            returned.append(Msg(rb.at[half, r], eret.at[me], dev(dz, dy, 0, half)).start())

    def results(ref):
        return jnp.concatenate([dot(ref[...], ed[...]), jnp.zeros((8, 512), F32)], axis=0)

    for m in eh_in:
        m.arrived()
    eo = results(eh)
    for r in range(7, -1, -1):
        for half in range(2):
            give_back(half, r, eo[half * 48 + r * 6 : half * 48 + r * 6 + 8])
    for m in el_in:
        m.arrived()
    eo = results(el)
    for half in range(2):
        give_back(half, 15, eo[96 + half * 8 : 104 + half * 8])
    for r in range(14, 7, -1):
        for half in range(2):
            give_back(half, r, eo[half * 48 + (r - 8) * 6 : half * 48 + (r - 8) * 6 + 8])

    early_sends = len(sent) - 52
    for cp in sent[:early_sends]:
        cp.wait_send()
    lane = lax.broadcasted_iota(jnp.int32, (48, 512), 1).astype(F32)
    sel = jnp.concatenate(
        [jnp.where(lane == scol[0:48, ch : ch + 1] + float(hf * 8), 1.0, 0.0) for hf in range(2) for ch in range(2)], axis=0
    ).astype(BF16)
    total = rsr[0].astype(F32)
    for r in range(1, 16):
        reduced[r].arrived()
        total = total + rsr[r].astype(F32)
    base = res[:, cols].astype(F32) + bw * total
    for m in returned:
        m.arrived()
    got = dot(sel, eret[...].reshape(512, 256))
    for hf in range(2):
        s = slice(hf * 256, hf * 256 + 256)
        first, second = got[hf * 96 : hf * 96 + 48], got[hf * 96 + 48 : hf * 96 + 96]
        out[:, s] = (base[:, s] + first * rwc[0:48, 0:1] + second * rwc[0:48, 1:2]).astype(BF16)

    for cp in sent[early_sends:]:
        cp.wait_send()


def layer_call(*args):
    vm = pl.BlockSpec(memory_space=pltpu.VMEM)
    args = [pltpu.with_memory_space_constraint(a, pltpu.HBM) for a in args]
    return pl.pallas_call(
        layer_kernel,
        out_shape=(
            jax.ShapeDtypeStruct((48, 512), BF16),
            jax.ShapeDtypeStruct((48, 2, 128, 128), F32),
            jax.ShapeDtypeStruct((96, 128), F32),
            jax.ShapeDtypeStruct((2, 48), F32),
        ),
        in_specs=[pl.BlockSpec(memory_space=pltpu.HBM)] * 24,
        out_specs=(vm, vm, vm, vm),
        scratch_shapes=[
            pltpu.SMEM((2,), F32),
            pltpu.SMEM((2,), F32),
            pltpu.VMEM((48, 2048), BF16),
            pltpu.VMEM((1, 2048), F32),
            pltpu.VMEM((4, 2048, 256), BF16),
            pltpu.VMEM((2, 2048), BF16),
            pltpu.VMEM((2, 2048), BF16),
            pltpu.VMEM((96, 128), F32),
            pltpu.VMEM((2, 48), F32),
            pltpu.VMEM((2, 48), jnp.int32),
            pltpu.VMEM((48, 2048), BF16),
            pltpu.VMEM((2, 144, 128), BF16),
            pltpu.VMEM((2, 48, 128), F32),
            pltpu.VMEM((2, 48, 128), F32),
            pltpu.VMEM((2, 128, 144), BF16),
            pltpu.VMEM((2, 128, 144), BF16),
            pltpu.VMEM((2, 48, 128), F32),
            pltpu.SemaphoreType.DMA((4,)),
            pltpu.SemaphoreType.DMA((N_CHUNK,)),
            pltpu.SemaphoreType.DMA((9,)),
            pltpu.VMEM((4, 48, 256), BF16),
            pltpu.VMEM((1024, 2048), BF16),
            pltpu.VMEM((1, 2048), F32),
            pltpu.VMEM((16, 128), BF16),
            pltpu.VMEM((48, 2048), F32),
            pltpu.VMEM((2, 48), F32),
            pltpu.VMEM((256, 2048), BF16),
            pltpu.VMEM((512, 512), BF16),
            pltpu.VMEM((2048, 256), BF16),
            pltpu.VMEM((2048, 256), BF16),
            pltpu.VMEM((1024, 512), BF16),
            pltpu.VMEM((16, 8, 128), F32),
            pltpu.VMEM((16, 4, 48, 512), BF16),
            pltpu.VMEM((48, 2048), BF16),
            pltpu.VMEM((768, 512), BF16),
            pltpu.VMEM((96, 2048), F32),
            pltpu.VMEM((96, 2048), F32),
            pltpu.VMEM((96, 2048), BF16),
            pltpu.VMEM((96, 2048), BF16),
            pltpu.VMEM((3, 8, 2048), F32),
            pltpu.VMEM((96, 1024), BF16),
            pltpu.VMEM((112, 1024), BF16),
            pltpu.VMEM((16, 48, 512), BF16),
            pltpu.VMEM((16, 48, 512), BF16),
            pltpu.VMEM((2, 16, 16, 256), BF16),
            pltpu.VMEM((32, 16, 256), BF16),
            pltpu.SemaphoreType.DMA((N_MSG,)),
            pltpu.SemaphoreType.DMA((N_MSG,)),
            pltpu.SemaphoreType.DMA((16,)),
        ],
        compiler_params=pltpu.CompilerParams(vmem_limit_bytes=44 * 2**20, collective_id=0, has_side_effects=True),
        name="layer",
    )(*args)


def finish_kernel(lay, cell, norm, mx, lay_o, cell_o, norm_o, max_o, sem):
    copies = [
        pltpu.make_async_copy(cell.at[12 * i : 12 * i + 12], cell_o.at[12 * i : 12 * i + 12], sem.at[i]) for i in range(4)
    ]
    copies.append(pltpu.make_async_copy(lay, lay_o, sem.at[4]))
    copies.append(pltpu.make_async_copy(norm, norm_o, sem.at[5]))
    copies.append(pltpu.make_async_copy(mx, max_o, sem.at[6]))
    for cp in copies:
        cp.start()
    for cp in copies:
        cp.wait()


def finish_call(*args):
    any_ = pl.BlockSpec(memory_space=pl.ANY)
    vm = pl.BlockSpec(memory_space=pltpu.VMEM)
    return pl.pallas_call(
        finish_kernel,
        out_shape=tuple(jax.ShapeDtypeStruct(a.shape, a.dtype) for a in args),
        in_specs=[vm] * 4,
        out_specs=[any_] * 4,
        scratch_shapes=[pltpu.SemaphoreType.DMA((7,))],
        compiler_params=pltpu.CompilerParams(vmem_limit_bytes=16 * 2**20),
        name="finish",
    )(*[pltpu.with_memory_space_constraint(a, pltpu.VMEM) for a in args])


def local(
    tokens, mix_gain, w_query, w_key, w_value, w_outgate, w_ingate, w_forget, in_bias, forget_bias, w_mix_out,
    cell_state, norm_state, max_state, moe_gain, route_ids, route_weights, expert_gate, expert_up, expert_down,
    branch_gate, dense_gate, dense_up, dense_down,
):
    parts = layer_call(
        tokens, mix_gain.reshape(1, 2048), w_query, w_key, w_value, w_outgate, w_ingate.T, w_forget.T,
        in_bias, forget_bias, cell_state, norm_state.reshape(96, 128), max_state.T, route_ids.T,
        w_mix_out, moe_gain.reshape(1, 2048), branch_gate.reshape(16, 128), route_weights.T,
        dense_gate.T, dense_up.T, dense_down,
        expert_gate.reshape(2048, 256), expert_up.reshape(2048, 256), expert_down.reshape(256, 2048),
    )
    layer_out, new_cell, new_norm, new_max = finish_call(*parts)
    return (layer_out, new_cell, new_norm.reshape(48, 2, 128), new_max.T)


def solution(mesh):
    in_specs = (
        P("ep", None),
        P(),
        P(None, "tp"),
        P(None, "tp"),
        P(None, "tp"),
        P(None, "tp"),
        P(None, "tp"),
        P(None, "tp"),
        P("tp"),
        P("tp"),
        P(),
        P("ep", "tp", None, None),
        P("ep", "tp", None),
        P("ep", "tp"),
        P(),
        P("ep", None),
        P("ep", None),
        P("ep", None, "tp"),
        P("ep", None, "tp"),
        P("ep", "tp", None),
        P(),
        P(None, ("ep", "tp")),
        P(None, ("ep", "tp")),
        P(("ep", "tp"), None),
    )
    out_specs = (P("ep", "tp"), P("ep", "tp", None, None), P("ep", "tp", None), P("ep", "tp"))
    return jax.shard_map(local, mesh=mesh, in_specs=in_specs, out_specs=out_specs, check_vma=False)
```

```python
import functools

import jax
import jax.numpy as jnp
from jax import lax
from jax.experimental import pallas as pl
from jax.experimental.pallas import tpu as pltpu
from jax.sharding import PartitionSpec as P

EPS = 1e-06
MESH = pl.DeviceIdType.MESH
F32 = jnp.float32
BF16 = jnp.bfloat16
NT = (((1,), (1,)), ((), ()))


def dot(a, b):
    return jnp.dot(a, b, preferred_element_type=F32)


def dot_nt(a, b):
    return lax.dot_general(a, b, NT, preferred_element_type=F32)


CHUNK = 12
N_CHUNK = 4


def split3(a):
    first = a.astype(BF16).astype(F32)
    rest = a - first
    second = rest.astype(BF16).astype(F32)
    return first, second, rest - second


def as_columns(rows):
    n, width = rows.shape
    wide = jnp.concatenate([rows, jnp.zeros((n, 128 - width), F32)], axis=1) if width < 128 else rows
    return jnp.concatenate([wide, jnp.zeros((128 - n, 128), F32)], axis=0).T


def slot_rows(ids):
    idf = ids.astype(F32)
    idc = as_columns(idf)
    before = lax.broadcasted_iota(jnp.int32, (48, 48), 0) < lax.broadcasted_iota(jnp.int32, (48, 48), 1)
    slots = []
    for ch in range(2):
        row = idf[ch : ch + 1, :]
        hits = jnp.where(idc[0:48, 0:1] == row, 1.0, 0.0) + jnp.where(idc[0:48, 1:2] == row, 1.0, 0.0)
        rank = jnp.sum(jnp.where(before, hits, 0.0), axis=0, keepdims=True)
        slots.append(row * 16.0 + rank)
    srow = jnp.concatenate(slots + [jnp.zeros((6, 48), F32)], axis=0)
    return jnp.concatenate([srow, jnp.zeros((8, 80), F32)], axis=1)


REL = [
    (0, 0), (1, 0), (3, 0), (0, 1), (0, 3),
    (1, 1), (1, 3), (3, 1), (3, 3), (2, 0), (0, 2),
    (2, 1), (2, 3), (1, 2), (3, 2),
    (2, 2),
]
IDX = {rel: i for i, rel in enumerate(REL)}
GROUPS = [(0, 5), (5, 6), (11, 4), (15, 1)]
ZP, ZM, YP, YM = (1, 0), (3, 0), (0, 1), (0, 3)
N_MSG = 160


def layer_kernel(
    tok_h, cgain_h, wq_h, wk_h, wv_h, wo_h, win_h, wf_h, inb_h, fb_h, cell_h, norm_h, max_h, ids_h,
    wmix_h, gain_h, bg_h, rw_h, gate_h, up_h, down_h, eg_h, eu_h, ed_h,
    out, cell, norm_o, max_o,
    inb, fb, tok, cgain, wts, win, wf, norm, mx, ids, normed, vs, vf, cb, qt, wt, num, wsem, csem, msem,
    ah, wmix, gain, bg, macc, rw, w, d, eg, eu, ed, meta, g, res, hid, xo, xp, xb, xs, xl, eh, el, sb, rsr, rb, eret,
    ssem, rsem, lsem,
):
    me = lax.axis_index("ep")
    x = lax.axis_index("tp")
    c = lax.rem(me, 2)
    zy = lax.div(me, 2)
    y = lax.rem(zy, 4)
    z = lax.div(zy, 4)

    def dev(dz, dy, dx, pc):
        zz = lax.rem(z + dz, 4)
        yy = lax.rem(y + dy, 4)
        cc = 1 - c if pc else c
        return ((zz * 4 + yy) * 2 + cc, lax.rem(x + dx, 4))

    count = [0]
    sent = []

    class Msg:
        def __init__(self, src, dst, device):
            n = count[0]
            count[0] += 1
            self.copy = pltpu.make_async_remote_copy(
                src_ref=src, dst_ref=dst, send_sem=ssem.at[n], recv_sem=rsem.at[n], device_id=device, device_id_type=MESH
            )

        def start(self):
            self.copy.start()
            sent.append(self.copy)
            return self

        def arrived(self):
            self.copy.wait_recv()

    local = []

    def load(src, dst):
        cp = pltpu.make_async_copy(src, dst, lsem.at[len(local)])
        local.append(cp)
        cp.start()
        return cp

    barrier = pltpu.get_barrier_semaphore()
    peers = [dev(0, 0, 1, 0), dev(0, 0, 2, 0), dev(0, 0, 3, 0), dev(0, 0, 0, 1)]
    peers += [dev(dz, dy, 0, 0) for dz, dy in (ZP, ZM, YP, YM, (2, 0), (0, 2))]
    here = y * 4 + z
    cols = pl.ds(pl.multiple_of(x * 512, 512), 512)

    small = [
        pltpu.make_async_copy(src, dst, msem.at[i])
        for i, (src, dst) in enumerate(
            [(tok_h, tok), (cgain_h, cgain), (win_h, win), (wf_h, wf), (max_h, mx), (norm_h, norm), (ids_h, ids), (inb_h, inb), (fb_h, fb)]
        )
    ]
    for cp in small[0:2]:
        cp.start()
    wcp = [pltpu.make_async_copy(src, wts.at[i], wsem.at[i]) for i, src in enumerate([wq_h, wk_h, wv_h, wo_h])]
    wcp[0].start()
    for cp in small[2:]:
        cp.start()
    for cp in wcp[1:]:
        cp.start()

    def cin(i):
        s = pl.ds(i * CHUNK, CHUNK)
        return pltpu.make_async_copy(cell_h.at[s], cell.at[s], csem.at[i])

    for peer in peers:
        pl.semaphore_signal(barrier, inc=1, device_id=peer, device_id_type=MESH)
    for cp in small[0:2]:
        cp.wait()
    for i in range(N_CHUNK):
        cin(i).start()
    xf = tok[...].astype(F32)
    ms = jnp.mean(xf * xf, axis=-1, keepdims=True)
    normed[...] = (xf * lax.rsqrt(ms + EPS) * cgain[...]).astype(BF16)
    nb = normed[...]
    for cp in small[2:]:
        cp.wait()
    meta[here] = slot_rows(ids[...])
    in_pre = dot_nt(win[...], nb)
    fpre = dot_nt(wf[...], nb)
    hrow = lax.broadcasted_iota(jnp.int32, in_pre.shape, 0)
    in_pre = in_pre + jnp.where(hrow == 0, inb[0], inb[1])
    fpre = fpre + jnp.where(hrow == 0, fb[0], fb[1])
    log_f = jnp.minimum(fpre, 0.0) - jnp.log1p(jnp.exp(-jnp.abs(fpre)))
    lm = log_f + mx[...]
    new_max = jnp.maximum(lm, in_pre)
    max_o[...] = new_max
    carry = jnp.exp(lm - new_max)
    write = jnp.exp(in_pre - new_max)
    floor = jnp.exp(-new_max)
    rows = jnp.concatenate([carry, write, floor], axis=0)
    rows = jnp.concatenate([rows, jnp.zeros((6, 80), F32)], axis=1)
    rows = jnp.concatenate([rows, jnp.zeros((122, 128), F32)], axis=0)
    gcols = rows.T

    for cp in wcp:
        cp.wait()
    q = dot(nb, wts[0])
    k = dot(nb, wts[1]) * (128 ** (-0.5))
    v = dot(nb, wts[2])
    for h in range(2):
        v1, v2, _ = split3(v[:, h * 128 : (h + 1) * 128])
        vs[h] = jnp.concatenate([v1, v1, v2], axis=0).astype(BF16)
        vf[h] = v[:, h * 128 : (h + 1) * 128]
    og = jax.nn.sigmoid(dot(nb, wts[3]))

    cp_wmix = load(wmix_h, wmix)
    cp_gain = load(gain_h, gain)
    cp_bg = load(bg_h, bg)
    cp_rw = load(rw_h, rw)
    cp_gate = load(gate_h, w.at[0:64])
    cp_up = load(up_h, w.at[128:192])
    cp_down = load(down_h.at[:, cols], d.at[0:64])
    cp_ed = load(ed_h.at[:, cols], ed.at[0:256])
    cp_eg = load(eg_h, eg)
    cp_eu = load(eu_h, eu)

    pl.semaphore_wait(barrier, len(peers))
    w_p = [
        Msg(gate_h, w.at[64:128], dev(0, 0, 0, 1)).start(),
        Msg(up_h, w.at[192:256], dev(0, 0, 0, 1)).start(),
    ]
    down_p = [Msg(down_h.at[:, cols], d.at[64:128], dev(0, 0, 0, 1)).start()]
    down_x, ed_x = {}, {}

    def their(dx):
        return pl.ds(pl.multiple_of(lax.rem(x + dx, 4) * 512, 512), 512)

    def send_ed(dx):
        s = (4 - dx) % 4
        ed_x[s] = Msg(ed_h.at[:, their(dx)], ed.at[s * 256 : s * 256 + 256], dev(0, 0, dx, 0)).start()

    m_z = [Msg(meta.at[here], meta.at[here], dev(dz, 0, 0, 0)).start() for dz in (2, 1, 3)]

    denom = []
    pad = jnp.zeros((112, 128), F32)
    for h in range(2):
        ca = jnp.broadcast_to(gcols[0:48, h : h + 1], (48, 128))
        wr = jnp.broadcast_to(gcols[0:48, 2 + h : 3 + h], (48, 128))
        qh = q[:, h * 128 : (h + 1) * 128]
        written = wr * k[:, h * 128 : (h + 1) * 128]
        hs = pl.ds(h, 48, stride=2)
        nn = ca * norm[hs, :] + written
        norm_o[hs, :] = nn
        den = jnp.sum(qh * nn, axis=-1, keepdims=True)
        denom.append(jnp.maximum(jnp.abs(den), gcols[0:48, 4 + h : 5 + h]))
        cb[h] = ca
        vf[h] = jnp.sum(qh * written, axis=-1, keepdims=True) * vf[h]
        q1, q2, q3 = split3(qh)
        qt[h] = jnp.concatenate([q1, q2, q3, pad], axis=0).T[:, 0:144].astype(BF16)
        w1, w2, _ = split3(written)
        wt[h] = jnp.concatenate([w1, w2, w1, pad], axis=0).T[:, 0:144].astype(BF16)

    token = lax.rem(lax.broadcasted_iota(jnp.int32, (144, 128), 0), 48)

    def tokens_of(i):
        return [token == i * CHUNK + j for j in range(CHUNK)]

    def read_step(i, _):
        cin(i).wait()
        ones = jnp.concatenate([jnp.where(m, 1.0, 0.0) for m in tokens_of(i)], axis=1).astype(BF16)
        for h in range(2):
            qcols = dot(qt[h], ones)
            for j in range(CHUNK):
                b = i * CHUNK + j
                num[h, pl.ds(b, 1), :] = jnp.sum(
                    qcols[:, j * 128 : (j + 1) * 128] * cell[b, h], axis=0, keepdims=True
                )
        return 0

    def write_step(i, _):
        here = tokens_of(i)
        for h in range(2):
            vh = vs[h].astype(F32)
            vrows = jnp.concatenate([jnp.where(m, vh, 0.0) for m in here], axis=1).astype(BF16)
            outer = dot(wt[h], vrows)
            for j in range(CHUNK):
                b = i * CHUNK + j
                cell[b, h] = cb[h, pl.ds(b, 1), :] * cell[b, h] + outer[:, j * 128 : (j + 1) * 128]
        return 0

    lax.fori_loop(0, N_CHUNK, read_step, 0)
    for h in range(2):
        lanes = slice(h * 128, (h + 1) * 128)
        ah[x, :, lanes] = (og[:, lanes] * ((cb[h] * num[h] + vf[h]) / denom[h])).astype(BF16)

    heads = {}
    for dx in (2, 1, 3):
        heads[(4 - dx) % 4] = Msg(ah.at[x], ah.at[x], dev(0, 0, dx, 0)).start()

    cp_wmix.wait()
    cp_gain.wait()
    cp_bg.wait()

    def head_part(s, n):
        src = lax.rem(x + s, 4)
        rows = pl.ds(pl.multiple_of(src * 256, 256), 256)
        return dot(ah[src], wmix[rows, n * 512 : (n + 1) * 512])

    for n in range(4):
        s = slice(n * 512, (n + 1) * 512)
        macc[:, s] = tok[:, s].astype(F32) + head_part(0, n)
    for h in (1, 3):
        heads[h].arrived()
        for n in range(4):
            macc[:, n * 512 : (n + 1) * 512] += head_part(h, n)
    heads[2].arrived()
    sq = jnp.zeros((48, 1), F32)
    for n in range(4):
        s = slice(n * 512, (n + 1) * 512)
        r = (macc[:, s] + head_part(2, n)).astype(BF16)
        res[:, s] = r
        rf = r.astype(F32)
        sq = sq + jnp.sum(rf * rf, axis=-1, keepdims=True)
    inv = lax.rsqrt(sq * (1.0 / 2048.0) + EPS)
    for n in range(4):
        s = slice(n * 512, (n + 1) * 512)
        g[0, n] = (res[:, s].astype(F32) * inv * gain[:, s]).astype(BF16)

    def spread(rel, q0, nq, way):
        to = ((rel[0] - way[0]) % 4, (rel[1] - way[1]) % 4)
        q = pl.ds(q0, nq)
        return Msg(g.at[IDX[rel], q], g.at[IDX[to], q], dev(*way, 0, 0)).start()

    O = (0, 0)
    a_zp, a_zm = spread(O, 0, 2, ZP), spread(O, 0, 2, ZM)
    b_yp, b_ym = spread(O, 2, 2, YP), spread(O, 2, 2, YM)
    for m in m_z:
        m.arrived()
    col = pl.ds(y * 4, 4)
    m_y = [Msg(meta.at[col], meta.at[col], dev(0, dy, 0, 0)).start() for dy in (2, 1, 3)]

    for dx in (2, 1, 3):
        s = (4 - dx) % 4
        down_x[s] = Msg(down_h.at[:, their(dx)], d.at[s * 128 : s * 128 + 64], dev(0, 0, dx, 0)).start()
    for dx in (2, 1, 3):
        send_ed(dx)

    lax.fori_loop(0, N_CHUNK // 2, write_step, 0)
    a_yp, a_ym = spread(O, 0, 2, YP), spread(O, 0, 2, YM)
    b_zp, b_zm = spread(O, 2, 2, ZP), spread(O, 2, 2, ZM)

    gate_sum = jnp.zeros((48, 1), F32)
    gate_rows = bg[...].astype(F32)
    for n in range(4):
        rowsum = jnp.zeros((48, 128), F32)
        for i in range(4):
            rowsum = rowsum + g[0, n, :, i * 128 : (i + 1) * 128].astype(F32) * gate_rows[n * 4 + i : n * 4 + i + 1]
        gate_sum = gate_sum + jnp.sum(rowsum, axis=-1, keepdims=True)
    bw = jax.nn.sigmoid(gate_sum)
    cp_rw.wait()
    scol = as_columns(meta[here])
    rwc = as_columns(rw[...])

    a_zp.arrived()
    f_z0 = spread((3, 0), 0, 1, ZP)
    t_33, t_31 = spread((3, 0), 0, 2, YP), spread((3, 0), 0, 2, YM)
    a_zm.arrived()
    f_z1 = spread((1, 0), 1, 1, ZM)
    t_13, t_11 = spread((1, 0), 0, 2, YP), spread((1, 0), 0, 2, YM)
    b_yp.arrived()
    f_y2 = spread((0, 3), 2, 1, YP)
    u_33, u_13 = spread((0, 3), 2, 2, ZP), spread((0, 3), 2, 2, ZM)
    b_ym.arrived()
    f_y3 = spread((0, 1), 3, 1, YM)
    u_31, u_11 = spread((0, 1), 2, 2, ZP), spread((0, 1), 2, 2, ZM)
    a_yp.arrived()
    f_y0 = spread((0, 3), 0, 1, YP)
    a_ym.arrived()
    f_y1 = spread((0, 1), 1, 1, YM)
    b_zp.arrived()
    f_z2 = spread((3, 0), 2, 1, ZP)
    b_zm.arrived()
    f_z3 = spread((1, 0), 3, 1, ZM)

    def up_group(n):
        r0, nb = GROUPS[n]
        acc = None
        for q in range(4):
            part = dot_nt(g[r0 : r0 + nb, q].reshape(nb * 48, 512), w[:, q * 512 : (q + 1) * 512])
            acc = part if acc is None else acc + part
        ga, up = acc[:, 0:128], acc[:, 128:256]
        rows = pl.ds(r0 * 48, nb * 48)
        hid[rows, 0:128] = (ga * jax.nn.sigmoid(ga) * up).astype(BF16)
        out = {}
        for dx in (2, 1, 3):
            s = (4 - dx) % 4
            out[s] = Msg(hid.at[rows, 0:128], hid.at[rows, s * 128 : s * 128 + 128], dev(0, 0, dx, 0)).start()
        return out

    e_mine = (me * 16).astype(F32)
    e_other = ((zy * 2 + (1 - c)) * 16).astype(F32)

    def pick_group(n):
        r0, nb = GROUPS[n]
        lane8 = lax.broadcasted_iota(jnp.int32, (8, 48), 0).astype(F32)
        code = jnp.concatenate([lane8 + e_mine, lane8 + e_other], axis=0)
        for r in range(r0, r0 + nb):
            dz, dy = REL[r]
            m = meta[lax.rem(y + dy, 4) * 4 + lax.rem(z + dz, 4)]
            hit = jnp.where(m[0:1, 0:48] == code, 1.0, 0.0) + jnp.where(m[1:2, 0:48] == code, 1.0, 0.0)
            hit = hit.astype(BF16)
            for q in range(4):
                picked = dot(hit, g[r, q])
                s = slice(q * 512, (q + 1) * 512)
                if r == 15:
                    xl[0, :, s] = picked[0:8]
                    xl[1, :, s] = picked[8:16]
                else:
                    xo[r * 6 : r * 6 + 6, s] = picked[0:6]
                    xp[r * 6 : r * 6 + 6, s] = picked[8:14]

    xo[88:96, :] = jnp.zeros((8, 2048), F32)
    xp[88:96, :] = jnp.zeros((8, 2048), F32)

    def pass_rows(a, b):
        rows = slice(a, b)
        xs[rows] = xp[rows].astype(BF16)
        return Msg(xs.at[rows], xb.at[rows], dev(0, 0, 0, 1)).start()

    cp_down.wait()
    for s in (1, 2, 3):
        down_x[s].arrived()
        own = slice(s * 128, s * 128 + 64)
        down_p.append(Msg(d.at[own], d.at[s * 128 + 64 : s * 128 + 128], dev(0, 0, 0, 1)).start())

    cp_gate.wait()
    cp_up.wait()
    for m in w_p:
        m.arrived()
    hid_in = {}
    hid_in[0] = up_group(0)
    for m in m_y:
        m.arrived()
    pick_group(0)
    lax.fori_loop(N_CHUNK // 2, N_CHUNK, write_step, 0)

    f_z0.arrived()
    f_z1.arrived()
    t_23, t_21 = spread((2, 0), 0, 2, YP), spread((2, 0), 0, 2, YM)
    f_y2.arrived()
    f_y3.arrived()
    u_32, u_12 = spread((0, 2), 2, 2, ZP), spread((0, 2), 2, 2, ZM)
    t_33.arrived()
    h_32a = spread((3, 3), 0, 1, YP)
    t_31.arrived()
    h_32b = spread((3, 1), 1, 1, YM)
    t_13.arrived()
    h_12a = spread((1, 3), 0, 1, YP)
    t_11.arrived()
    h_12b = spread((1, 1), 1, 1, YM)
    u_33.arrived()
    h_23a = spread((3, 3), 2, 1, ZP)
    u_13.arrived()
    h_23b = spread((1, 3), 3, 1, ZM)
    u_31.arrived()
    h_21a = spread((3, 1), 2, 1, ZP)
    u_11.arrived()
    h_21b = spread((1, 1), 3, 1, ZM)
    for m in (f_y0, f_y1, f_z2, f_z3):
        m.arrived()

    reduced = {}

    def down_group(n):
        r0, nb = GROUPS[n]
        for m in hid_in[n].values():
            m.arrived()
        part = dot(hid[r0 * 48 : (r0 + nb) * 48, :], d[...])
        for i in range(nb):
            r = r0 + i
            blk = part[i * 48 : (i + 1) * 48].astype(BF16)
            if r == 0:
                rsr[0] = blk
            else:
                dz, dy = REL[r]
                sb[r] = blk
                back = IDX[((-dz) % 4, (-dy) % 4)]
                reduced[back] = Msg(sb.at[r], rsr.at[back], dev(dz, dy, 0, 0)).start()

    hid_in[1] = up_group(1)

    pick_group(1)
    first_rows = pass_rows(0, 48)

    t_23.arrived()
    l_22a = spread((2, 3), 0, 1, YP)
    t_21.arrived()
    l_22b = spread((2, 1), 1, 1, YM)
    u_32.arrived()
    l_22c = spread((3, 2), 2, 1, ZP)
    u_12.arrived()
    l_22d = spread((1, 2), 3, 1, ZM)

    for m in down_p:
        m.arrived()
    down_group(0)
    for m in (h_32a, h_32b, h_12a, h_12b, h_23a, h_23b, h_21a, h_21b):
        m.arrived()
    hid_in[2] = up_group(2)
    pick_group(2)
    second_rows = pass_rows(48, 96)

    cp_eg.wait()
    cp_eu.wait()

    def expert_up(ref, rows_in):
        ga = dot(rows_in, eg[...])
        up = dot(rows_in, eu[...])
        ref[:, 0:256] = (ga * jax.nn.sigmoid(ga) * up).astype(BF16)
        out = []
        for dx in (2, 1, 3):
            s = (4 - dx) % 4
            out.append(Msg(ref.at[:, 0:256], ref.at[:, s * 256 : s * 256 + 256], dev(0, 0, dx, 0)).start())
        return out

    first_rows.arrived()
    eh_in = expert_up(eh, jnp.concatenate([xo[0:48].astype(BF16), xb[0:48]], axis=0))

    for m in (l_22a, l_22b, l_22c, l_22d):
        m.arrived()
    pick_group(3)
    last_rows = Msg(xl.at[1], xl.at[2], dev(0, 0, 0, 1)).start()
    hid_in[3] = up_group(3)
    down_group(1)
    second_rows.arrived()
    el_in = expert_up(el.at[0:96], jnp.concatenate([xo[48:96].astype(BF16), xb[48:96]], axis=0))
    down_group(2)
    last_rows.arrived()
    el_in += expert_up(el.at[96:112], jnp.concatenate([xl[0], xl[2]], axis=0).astype(BF16))
    down_group(3)

    cp_ed.wait()
    for m in ed_x.values():
        m.arrived()
    returned = []

    def give_back(half, r, eo):
        blk = jnp.concatenate([eo[:, 0:256], eo[:, 256:512]], axis=0).astype(BF16)
        if r == 0 and half == 0:
            eret[me] = blk
        else:
            dz, dy = REL[r]
            rb[half, r] = blk
            returned.append(Msg(rb.at[half, r], eret.at[me], dev(dz, dy, 0, half)).start())

    def results(ref):
        return jnp.concatenate([dot(ref[...], ed[...]), jnp.zeros((8, 512), F32)], axis=0)

    for m in eh_in:
        m.arrived()
    eo = results(eh)
    for r in range(7, -1, -1):
        for half in range(2):
            give_back(half, r, eo[half * 48 + r * 6 : half * 48 + r * 6 + 8])
    for m in el_in:
        m.arrived()
    eo = results(el)
    for half in range(2):
        give_back(half, 15, eo[96 + half * 8 : 104 + half * 8])
    for r in range(14, 7, -1):
        for half in range(2):
            give_back(half, r, eo[half * 48 + (r - 8) * 6 : half * 48 + (r - 8) * 6 + 8])

    early_sends = len(sent) - 52
    for cp in sent[:early_sends]:
        cp.wait_send()
    lane = lax.broadcasted_iota(jnp.int32, (48, 512), 1).astype(F32)
    sel = jnp.concatenate(
        [jnp.where(lane == scol[0:48, ch : ch + 1] + float(hf * 8), 1.0, 0.0) for hf in range(2) for ch in range(2)], axis=0
    ).astype(BF16)
    total = rsr[0].astype(F32)
    for r in range(1, 16):
        reduced[r].arrived()
        total = total + rsr[r].astype(F32)
    base = res[:, cols].astype(F32) + bw * total
    for m in returned:
        m.arrived()
    got = dot(sel, eret[...].reshape(512, 256))
    for hf in range(2):
        s = slice(hf * 256, hf * 256 + 256)
        first, second = got[hf * 96 : hf * 96 + 48], got[hf * 96 + 48 : hf * 96 + 96]
        out[:, s] = (base[:, s] + first * rwc[0:48, 0:1] + second * rwc[0:48, 1:2]).astype(BF16)

    for cp in sent[early_sends:]:
        cp.wait_send()


def layer_call(*args):
    vm = pl.BlockSpec(memory_space=pltpu.VMEM)
    args = [pltpu.with_memory_space_constraint(a, pltpu.HBM) for a in args]
    return pl.pallas_call(
        layer_kernel,
        out_shape=(
            jax.ShapeDtypeStruct((48, 512), BF16),
            jax.ShapeDtypeStruct((48, 2, 128, 128), F32),
            jax.ShapeDtypeStruct((96, 128), F32),
            jax.ShapeDtypeStruct((2, 48), F32),
        ),
        in_specs=[pl.BlockSpec(memory_space=pltpu.HBM)] * 24,
        out_specs=(vm, vm, vm, vm),
        scratch_shapes=[
            pltpu.SMEM((2,), F32),
            pltpu.SMEM((2,), F32),
            pltpu.VMEM((48, 2048), BF16),
            pltpu.VMEM((1, 2048), F32),
            pltpu.VMEM((4, 2048, 256), BF16),
            pltpu.VMEM((2, 2048), BF16),
            pltpu.VMEM((2, 2048), BF16),
            pltpu.VMEM((96, 128), F32),
            pltpu.VMEM((2, 48), F32),
            pltpu.VMEM((2, 48), jnp.int32),
            pltpu.VMEM((48, 2048), BF16),
            pltpu.VMEM((2, 144, 128), BF16),
            pltpu.VMEM((2, 48, 128), F32),
            pltpu.VMEM((2, 48, 128), F32),
            pltpu.VMEM((2, 128, 144), BF16),
            pltpu.VMEM((2, 128, 144), BF16),
            pltpu.VMEM((2, 48, 128), F32),
            pltpu.SemaphoreType.DMA((4,)),
            pltpu.SemaphoreType.DMA((N_CHUNK,)),
            pltpu.SemaphoreType.DMA((9,)),
            pltpu.VMEM((4, 48, 256), BF16),
            pltpu.VMEM((1024, 2048), BF16),
            pltpu.VMEM((1, 2048), F32),
            pltpu.VMEM((16, 128), BF16),
            pltpu.VMEM((48, 2048), F32),
            pltpu.VMEM((2, 48), F32),
            pltpu.VMEM((256, 2048), BF16),
            pltpu.VMEM((512, 512), BF16),
            pltpu.VMEM((2048, 256), BF16),
            pltpu.VMEM((2048, 256), BF16),
            pltpu.VMEM((1024, 512), BF16),
            pltpu.VMEM((16, 8, 128), F32),
            pltpu.VMEM((16, 4, 48, 512), BF16),
            pltpu.VMEM((48, 2048), BF16),
            pltpu.VMEM((768, 512), BF16),
            pltpu.VMEM((96, 2048), F32),
            pltpu.VMEM((96, 2048), F32),
            pltpu.VMEM((96, 2048), BF16),
            pltpu.VMEM((96, 2048), BF16),
            pltpu.VMEM((3, 8, 2048), F32),
            pltpu.VMEM((96, 1024), BF16),
            pltpu.VMEM((112, 1024), BF16),
            pltpu.VMEM((16, 48, 512), BF16),
            pltpu.VMEM((16, 48, 512), BF16),
            pltpu.VMEM((2, 16, 16, 256), BF16),
            pltpu.VMEM((32, 16, 256), BF16),
            pltpu.SemaphoreType.DMA((N_MSG,)),
            pltpu.SemaphoreType.DMA((N_MSG,)),
            pltpu.SemaphoreType.DMA((16,)),
        ],
        compiler_params=pltpu.CompilerParams(vmem_limit_bytes=44 * 2**20, collective_id=0, has_side_effects=True),
        name="layer",
    )(*args)


def finish_kernel(lay, cell, norm, mx, lay_o, cell_o, norm_o, max_o, sem):
    copies = [
        pltpu.make_async_copy(cell.at[12 * i : 12 * i + 12], cell_o.at[12 * i : 12 * i + 12], sem.at[i]) for i in range(4)
    ]
    copies.append(pltpu.make_async_copy(lay, lay_o, sem.at[4]))
    copies.append(pltpu.make_async_copy(norm, norm_o, sem.at[5]))
    copies.append(pltpu.make_async_copy(mx, max_o, sem.at[6]))
    for cp in copies:
        cp.start()
    for cp in copies:
        cp.wait()


def finish_call(*args):
    any_ = pl.BlockSpec(memory_space=pl.ANY)
    vm = pl.BlockSpec(memory_space=pltpu.VMEM)
    return pl.pallas_call(
        finish_kernel,
        out_shape=tuple(jax.ShapeDtypeStruct(a.shape, a.dtype) for a in args),
        in_specs=[vm] * 4,
        out_specs=[any_] * 4,
        scratch_shapes=[pltpu.SemaphoreType.DMA((7,))],
        compiler_params=pltpu.CompilerParams(vmem_limit_bytes=16 * 2**20),
        name="finish",
    )(*[pltpu.with_memory_space_constraint(a, pltpu.VMEM) for a in args])


def local(
    tokens, mix_gain, w_query, w_key, w_value, w_outgate, w_ingate, w_forget, in_bias, forget_bias, w_mix_out,
    cell_state, norm_state, max_state, moe_gain, route_ids, route_weights, expert_gate, expert_up, expert_down,
    branch_gate, dense_gate, dense_up, dense_down,
):
    parts = layer_call(
        tokens, mix_gain.reshape(1, 2048), w_query, w_key, w_value, w_outgate, w_ingate.T, w_forget.T,
        in_bias, forget_bias, cell_state, norm_state.reshape(96, 128), max_state.T, route_ids.T,
        w_mix_out, moe_gain.reshape(1, 2048), branch_gate.reshape(16, 128), route_weights.T,
        dense_gate.T, dense_up.T, dense_down,
        expert_gate.reshape(2048, 256), expert_up.reshape(2048, 256), expert_down.reshape(256, 2048),
    )
    layer_out, new_cell, new_norm, new_max = finish_call(*parts)
    return (layer_out, new_cell, new_norm.reshape(48, 2, 128), new_max.T)


def solution(mesh):
    in_specs = (
        P("ep", None),
        P(),
        P(None, "tp"),
        P(None, "tp"),
        P(None, "tp"),
        P(None, "tp"),
        P(None, "tp"),
        P(None, "tp"),
        P("tp"),
        P("tp"),
        P(),
        P("ep", "tp", None, None),
        P("ep", "tp", None),
        P("ep", "tp"),
        P(),
        P("ep", None),
        P("ep", None),
        P("ep", None, "tp"),
        P("ep", None, "tp"),
        P("ep", "tp", None),
        P(),
        P(None, ("ep", "tp")),
        P(None, ("ep", "tp")),
        P(("ep", "tp"), None),
    )
    out_specs = (P("ep", "tp"), P("ep", "tp", None, None), P("ep", "tp", None), P("ep", "tp"))
    return jax.shard_map(local, mesh=mesh, in_specs=in_specs, out_specs=out_specs, check_vma=False)
```
